512 devices in a mesh: ep: 32 (over z, core), tp: 16 (over y, x).
Axes of the slice: x: 4, y: 4, z: 16, core: 2. Of those that a mesh axis runs over, the one named last changes fastest.
Arguments:
- hidden: bfloat16 [384, 2048], P('ep'), may hold values from -6 to 6
- pre_gain: bfloat16 [2048], replicated, may hold values from 0.099609375 to 1.8984375
- query_weight: bfloat16 [2048, 1024], P('ep', 'tp'), may hold values from -0.125 to 0.125
- key_cache: bfloat16 [384, 1024, 1024], P('ep', 'tp'), may hold values from -6 to 6
- value_cache: bfloat16 [384, 1024, 1024], P('ep', 'tp'), may hold values from -6 to 6
- lengths: int32 [384], P('ep'), may hold values from 128 to 1024
- stick_bias: float32 [16], P('tp'), may hold values from -8.5 to -3
- out_weight: bfloat16 [1024, 2048], P('tp', 'ep'), may hold values from -0.1875 to 0.1875
- post_gain: bfloat16 [2048], replicated, may hold values from 0.099609375 to 1.8984375
- ffn_gain: bfloat16 [2048], replicated, may hold values from 0.099609375 to 1.8984375
- expert_ids: int32 [384, 2], P('ep'), may hold values from 0 to 31, as said below
- route_logits: float32 [384, 2], P('ep'), may hold values from -6 to 6
- gate_experts: bfloat16 [32, 2048, 2048], P('ep', None, 'tp'), may hold values from -0.125 to 0.125
- up_experts: bfloat16 [32, 2048, 2048], P('ep', None, 'tp'), may hold values from -0.125 to 0.125
- down_experts: bfloat16 [32, 2048, 2048], P('ep', 'tp'), may hold values from -2 to 2
- out_gain: bfloat16 [2048], P('tp'), may hold values from 0.099609375 to 1.8984375
Outputs:
- result: bfloat16 [384, 2048], P('ep', 'tp')
The draws below stay inside these ranges and needn't reach their ends.
Inputs may be any that keep to these rules, and one draw needn't show every extreme that they name: `expert_ids`: each row names 2 different experts of one group of 4 consecutive experts. Among the rows of one device (aligned blocks of 12 rows) no expert is named more than 2 times, and one expert is named exactly 2 times in every block.
All inputs are finite; a program needn't handle non-finite values.
Results may differ from the reference program's by a relative error of at most 0.014.
Values may be sent and summed in bfloat16 or wider, within the bound.
A program may use at most 64 MiB of HBM per device.

```python
import jax
import jax.numpy as jnp
from jax import lax

D = 2048
HEADS = 16
HEAD = 64
FF = 2048
EXPERTS = 32
EXP_GROUP = 4
TOPK = 2
CACHE = 1024
SEQ_DEV = 12
TOKENS = 384
CAP = 2
N_EP = 32


def draw_expert_ids(key, part):
    groups = EXPERTS // EXP_GROUP
    blocks = TOKENS // SEQ_DEV
    slot_count = groups * CAP
    subkeys = jax.random.split(jax.random.fold_in(key, 11), 6)
    full_group = jax.random.randint(subkeys[0], (), 0, groups)
    full_first = jax.random.randint(subkeys[1], (), 0, EXP_GROUP)
    slot_group = jnp.arange(slot_count, dtype=jnp.int32) // CAP
    scores = jax.random.randint(subkeys[2], (blocks, slot_count), 0, 1 << 20) * slot_count + jnp.arange(slot_count, dtype=jnp.int32)[None, :]
    scores = jnp.where(slot_group[None, :] == full_group, scores - (1 << 26), scores)
    ranking = jnp.argsort(scores, axis=1)[:, :SEQ_DEV]
    chosen = slot_group[ranking]
    shuffle_scores = jax.random.randint(subkeys[3], (blocks, SEQ_DEV), 0, 1 << 20) * SEQ_DEV + jnp.arange(SEQ_DEV, dtype=jnp.int32)[None, :]
    shuffle = jnp.argsort(shuffle_scores, axis=1)
    group_of = jnp.take_along_axis(chosen, shuffle, axis=1)
    first_pick = jax.random.randint(subkeys[4], (blocks, SEQ_DEV), 0, EXP_GROUP)
    first_pick = jnp.where(group_of == full_group, full_first, first_pick)
    offset = jax.random.randint(subkeys[5], (blocks, SEQ_DEV), 1, EXP_GROUP)
    second = (first_pick + offset) % EXP_GROUP
    chosen_ids = jnp.stack([first_pick, second], axis=2) + group_of[:, :, None] * EXP_GROUP
    return chosen_ids.reshape(TOKENS, TOPK).astype(jnp.int32)


def draw_down_experts(key, part):
    base = jax.random.normal(jax.random.fold_in(key, 23), (EXPERTS, FF, D), jnp.float32) * FF ** (-0.5)
    column = jnp.arange(D, dtype=jnp.float32) / D
    column_scale = jnp.exp(jnp.log(10.0) * column) * 0.3
    values = jnp.clip(base * column_scale[None, None, :], -2.0, 2.0)
    return values.astype(jnp.bfloat16)


def place_ends(array, rng, least, high):
    extent = array.shape
    index_at = [jax.random.randint(jax.random.fold_in(rng, axis), (), 0, extent[axis]) for axis in range(len(extent))]
    array = array.at[tuple(index_at)].set(least)
    longest = extent.index(max(extent))
    index_at[longest] = (index_at[longest] + 1) % extent[longest]
    return array.at[tuple(index_at)].set(high)


def steps_of(stream_key, shape, shards, smallest, top_value):
    gain, own = 1.0, jax.random.fold_in(stream_key, 6)
    for axis_at, parts in shards:
        heights = jnp.exp(jax.random.uniform(jax.random.fold_in(own, axis_at), (parts,), jnp.float32, smallest / len(shards), top_value / len(shards)))
        gain = gain * jnp.repeat(heights, shape[axis_at] // parts).reshape([-1 if axis == axis_at else 1 for axis in range(len(shape))])
    return gain


def normal_values(stream_key, shape, deviation, bound, cuts=(), kind=jnp.bfloat16):
    values = jax.random.normal(stream_key, shape, jnp.float32) * deviation
    if len(cuts) > 0:
        values = steps_of(stream_key, shape, cuts, -0.22, 0.18) * values
    return jnp.clip(values, min=-bound, max=bound).astype(kind)


def setup_inputs(seed: int = 0) -> dict:
    splits = jax.random.split(jax.random.key(seed), 17)
    hidden = normal_values(splits[0], (TOKENS, D), 1.0, 6.0, ((0, 32),))
    pre_gain = jnp.clip(1.0 + 0.18 * jax.random.normal(splits[1], (D,), jnp.float32), 0.099609375, 1.8984375).astype(jnp.bfloat16)
    query_weight = normal_values(splits[2], (D, HEADS * HEAD), D ** -0.5, 0.125, ((0, 32), (1, 16)))
    key_cache = normal_values(splits[3], (TOKENS, HEADS * HEAD, CACHE), 1.0, 6.0, ((0, 32), (1, 16)))
    value_cache = normal_values(splits[4], (TOKENS, HEADS * HEAD, CACHE), 1.0, 6.0, ((0, 32), (1, 16)))
    lengths = place_ends(jax.random.randint(splits[5], (TOKENS,), CACHE // 8, CACHE + 1), jax.random.fold_in(splits[5], 1), CACHE // 8, CACHE).astype(jnp.int32)
    stick_bias = jnp.clip(-8.5 + 5.5 * jax.random.uniform(splits[6], (HEADS,), jnp.float32) ** steps_of(splits[6], (HEADS,), ((0, 16),), -0.2, 0.2), -8.5, -3.0)
    out_weight = normal_values(splits[7], (HEADS * HEAD, D), (HEADS * HEAD) ** -0.5, 0.1875, ((0, 16), (1, 32)))
    post_gain = jnp.clip(1.0 + 0.18 * jax.random.normal(splits[8], (D,), jnp.float32), 0.099609375, 1.8984375).astype(jnp.bfloat16)
    ffn_gain = jnp.clip(1.0 + 0.18 * jax.random.normal(splits[9], (D,), jnp.float32), 0.099609375, 1.8984375).astype(jnp.bfloat16)
    expert_ids = draw_expert_ids(jax.random.fold_in(splits[16], 71), 0)
    route_logits = normal_values(splits[11], (TOKENS, TOPK), 1.5, 6.0, ((0, 32),), jnp.float32)
    gate_experts = normal_values(splits[12], (EXPERTS, D, FF), D ** -0.5, 0.125, ((0, 32), (2, 16)))
    up_experts = normal_values(splits[13], (EXPERTS, D, FF), D ** -0.5, 0.125, ((0, 32), (2, 16)))
    down_experts = draw_down_experts(jax.random.fold_in(splits[16], 71), 0)
    out_gain = jnp.clip(1.0 + 0.18 * jax.random.normal(splits[15], (D,), jnp.float32), 0.099609375, 1.8984375).astype(jnp.bfloat16)
    return {"hidden": hidden, "pre_gain": pre_gain, "query_weight": query_weight, "key_cache": key_cache, "value_cache": value_cache, "lengths": lengths, "stick_bias": stick_bias, "out_weight": out_weight, "post_gain": post_gain, "ffn_gain": ffn_gain, "expert_ids": expert_ids, "route_logits": route_logits, "gate_experts": gate_experts, "up_experts": up_experts, "down_experts": down_experts, "out_gain": out_gain}


epsilon = 1e-06

def inverse_rms(squares, features):
    return lax.rsqrt(squares / features + epsilon)

def stick_read(queries, key_blocks, value_blocks, lengths, head_bias):
    sequences, heads, head_size = queries.shape
    positions = key_blocks.shape[3]
    scores = jnp.einsum('she,shec->shc', queries.astype(jnp.float32), key_blocks.astype(jnp.float32))
    scores = scores * head_size ** (-0.5) + head_bias[None, :, None]
    places = lax.broadcasted_iota(jnp.int32, (sequences, heads, positions), 2)
    inside = places < lengths[:, None, None]
    log_fail = jnp.where(inside, jax.nn.log_sigmoid(-scores), 0.0)
    after_sum = lax.cumsum(log_fail, axis=2, reverse=True) - log_fail
    weight = jnp.where(inside, jnp.exp(jax.nn.log_sigmoid(scores) + after_sum), 0.0).astype(jnp.bfloat16)
    weight = lax.optimization_barrier(weight).astype(jnp.float32)
    mixed_heads = jnp.einsum('shc,shec->she', weight, value_blocks.astype(jnp.float32))
    return mixed_heads.astype(jnp.bfloat16)

def reference(hidden, pre_gain, query_weight, key_cache, value_cache, lengths, stick_bias, out_weight, post_gain, ffn_gain, expert_ids, route_logits, gate_experts, up_experts, down_experts, out_gain):
    hidden_wide = hidden.astype(jnp.float32)
    normed = (hidden_wide * inverse_rms(lax.optimization_barrier(jnp.sum(hidden_wide * hidden_wide, axis=1, keepdims=True)), D) * pre_gain.astype(jnp.float32)).astype(jnp.bfloat16)
    queries = jnp.dot(normed, query_weight, preferred_element_type=jnp.float32).astype(jnp.bfloat16)
    queries = queries.reshape(TOKENS, HEADS, HEAD)
    key_blocks = key_cache.reshape(TOKENS, HEADS, HEAD, CACHE)
    value_blocks = value_cache.reshape(TOKENS, HEADS, HEAD, CACHE)

    def one_head(head_index):
        query_head = lax.dynamic_slice_in_dim(queries, head_index, 1, 1)
        key_head = lax.dynamic_slice_in_dim(key_blocks, head_index, 1, 1)
        value_head = lax.dynamic_slice_in_dim(value_blocks, head_index, 1, 1)
        bias_head = lax.dynamic_slice_in_dim(stick_bias, head_index, 1, 0)
        return stick_read(query_head, key_head, value_head, lengths, bias_head)[:, 0, :]
    mixed_heads = lax.map(one_head, jnp.arange(HEADS, dtype=jnp.int32))
    mixed_heads = jnp.transpose(mixed_heads, (1, 0, 2)).reshape(TOKENS, HEADS * HEAD)
    attended = jnp.dot(mixed_heads, out_weight, preferred_element_type=jnp.float32).astype(jnp.bfloat16)
    attended = lax.optimization_barrier(attended).astype(jnp.float32)
    residual = (hidden_wide + attended * inverse_rms(lax.optimization_barrier(jnp.sum(attended * attended, axis=1, keepdims=True)), D) * post_gain.astype(jnp.float32)).astype(jnp.bfloat16)
    residual_wide = residual.astype(jnp.float32)
    ffn_in = (residual_wide * inverse_rms(lax.optimization_barrier(jnp.sum(residual_wide * residual_wide, axis=1, keepdims=True)), D) * ffn_gain.astype(jnp.float32)).astype(jnp.bfloat16)
    flat_ids = expert_ids.reshape(N_EP, SEQ_DEV * TOPK)
    choose = (flat_ids[:, :, None] == jnp.arange(EXPERTS, dtype=jnp.int32)[None, None, :]).astype(jnp.int32)
    earlier = jnp.cumsum(choose, axis=1) - choose
    slot_of = lax.optimization_barrier(jnp.sum(earlier * choose, axis=2))
    source = jnp.broadcast_to(jnp.arange(N_EP, dtype=jnp.int32)[:, None], slot_of.shape)
    token_of = source * SEQ_DEV + jnp.broadcast_to((jnp.arange(SEQ_DEV * TOPK, dtype=jnp.int32) // TOPK)[None, :], slot_of.shape)
    row_table = jnp.full((EXPERTS, N_EP, CAP), TOKENS, jnp.int32).at[flat_ids, source, slot_of].set(token_of)
    padded = jnp.concatenate([ffn_in, jnp.zeros((1, D), jnp.bfloat16)], axis=0)

    def one_expert(expert):
        expert_rows = padded[row_table[expert].reshape(-1)]
        gate_act = jnp.dot(expert_rows, gate_experts[expert], preferred_element_type=jnp.float32)
        up_act = jnp.dot(expert_rows, up_experts[expert], preferred_element_type=jnp.float32)
        active = (jax.nn.silu(gate_act) * up_act).astype(jnp.bfloat16)
        return jnp.dot(active, down_experts[expert], preferred_element_type=jnp.float32).astype(jnp.bfloat16)
    outputs = lax.map(one_expert, jnp.arange(EXPERTS, dtype=jnp.int32))
    where_row = (source * CAP + slot_of).reshape(TOKENS, TOPK)
    picked = outputs[expert_ids, where_row].astype(jnp.float32)
    route_weight = jax.nn.softmax(route_logits.astype(jnp.float32), axis=1)
    combined = lax.optimization_barrier(jnp.sum(route_weight[:, :, None] * picked, axis=1))
    result = residual_wide + combined * inverse_rms(lax.optimization_barrier(jnp.sum(combined * combined, axis=1, keepdims=True)), D) * out_gain.astype(jnp.float32)
    return result.astype(jnp.bfloat16)
```

```python
import functools

import jax
import jax.numpy as jnp
from jax import lax
from jax.experimental import pallas as pl
from jax.experimental.pallas import tpu as pltpu
from jax.sharding import PartitionSpec as P

epsilon = 1e-06
F32 = jnp.float32
BF16 = jnp.bfloat16
MESH = pl.DeviceIdType.MESH
NT = (((1,), (1,)), ((), ()))


def iota(shape, dim):
    return lax.broadcasted_iota(jnp.int32, shape, dim)


def inverse_rms(squares, features):
    return lax.rsqrt(squares / features + epsilon)


def eye(n):
    return (iota((n, n), 0) == iota((n, n), 1)).astype(BF16)


def transposed(value):
    return lax.dot_general(
        eye(value.shape[1]), value.astype(BF16), NT, preferred_element_type=F32
    )


def three_parts(value):
    high = value.astype(BF16)
    rest = value - high.astype(F32)
    middle = rest.astype(BF16)
    low = (rest - middle.astype(F32)).astype(BF16)
    return high, middle, low


def layer_kernel(
    ep_count,
    tp_count,
    hidden_ref,
    pre_gain_ref,
    query_weight_ref,
    key_hbm,
    value_hbm,
    lengths_ref,
    stick_bias_ref,
    out_weight_ref,
    post_gain_ref,
    ffn_gain_ref,
    expert_ids_ref,
    route_logits_ref,
    gate_hbm,
    up_hbm,
    down_hbm,
    out_gain_ref,
    result_ref,
    keys,
    values,
    gates,
    ups,
    downs,
    wq_all,
    wo_all,
    wo_full,
    scores_scr,
    stick_scr,
    place_scr,
    mix_scr,
    ids_scr,
    logits_scr,
    own_scr,
    gain_scr,
    tri_scr,
    rs_out,
    rs_in,
    hz_out,
    hz_in,
    az_out,
    az_in,
    h_rows,
    a_rows,
    r_scr,
    f_scr,
    ex_out,
    ex_in,
    back_out,
    back_in,
    asq_in,
    csq_in,
    load_sem,
    wq_recv,
    wo_recv,
    recv_sem,
    send_sem,
):
    me = lax.axis_index("ep")
    mine = lax.axis_index("tp")
    place = me // 2
    core = lax.rem(me, 2)
    partner = me + 1 - 2 * core
    chips = ep_count // 2
    half = chips // 2
    sequences, features = hidden_ref.shape
    padded = 16
    positions = keys.shape[2]
    head_size = keys.shape[1]
    width = features // tp_count
    blocks = positions // 128

    barrier = pltpu.get_barrier_semaphore()

    def greet_ep(d, carry):
        pl.semaphore_signal(
            barrier, inc=1, device_id=(lax.rem(me + d, ep_count), mine), device_id_type=MESH
        )
        return carry

    def greet_tp(d, carry):
        pl.semaphore_signal(
            barrier, inc=1, device_id=(me, lax.rem(mine + d, tp_count)), device_id_type=MESH
        )
        return carry

    lax.fori_loop(1, ep_count, greet_ep, 0)
    lax.fori_loop(1, tp_count, greet_tp, 0)

    loads = [
        pltpu.make_async_copy(key_hbm, keys, load_sem.at[0]),
        pltpu.make_async_copy(value_hbm, values, load_sem.at[1]),
        pltpu.make_async_copy(gate_hbm.at[0], gates, load_sem.at[2]),
        pltpu.make_async_copy(up_hbm.at[0], ups, load_sem.at[3]),
        pltpu.make_async_copy(down_hbm.at[0], downs, load_sem.at[4]),
    ]
    for load in loads:
        load.start()

    wq = query_weight_ref[...].astype(F32)
    rows_half = wq.shape[0] // 2
    wq_all[me, 0] = jnp.concatenate([wq[:rows_half], wq[rows_half:]], axis=1).astype(BF16)
    wo = out_weight_ref[...].astype(F32)
    wo_half = wo.shape[0] // 2
    wo_all[me] = jnp.concatenate([wo[:wo_half], wo[wo_half:]], axis=1).astype(BF16)

    hidden = hidden_ref[...].astype(F32)
    normed = (
        hidden
        * inverse_rms(jnp.sum(hidden * hidden, axis=1, keepdims=True), features)
        * pre_gain_ref[...].astype(F32).reshape(1, features)
    ).astype(BF16)

    own_columns = pl.ds(pl.multiple_of(mine * width, width), width)
    own_scr[...] = jnp.zeros_like(own_scr)
    own_scr[0:sequences, :] = hidden_ref[:, own_columns].astype(F32)
    ids_scr[...] = jnp.full(ids_scr.shape, -1, jnp.int32)
    ids_scr[0:sequences, :] = expert_ids_ref[...]
    logits_scr[...] = jnp.zeros_like(logits_scr)
    logits_scr[0:sequences, :] = route_logits_ref[...]
    scores_scr[...] = jnp.zeros_like(scores_scr)
    post_gain = post_gain_ref[...].astype(F32).reshape(1, features)
    for c in range(tp_count):
        gain_scr[c] = post_gain[:, width * c : width * c + width]

    ids = ids_scr[...]
    lanes = iota((padded, ep_count), 1)
    picks = [(ids[:, k : k + 1] == lanes).astype(F32) for k in range(2)]
    either = picks[0] + picks[1]
    before = (iota((padded, padded), 1) < iota((padded, padded), 0)).astype(BF16)
    earlier = jnp.dot(before, either.astype(BF16), preferred_element_type=F32)
    logits = logits_scr[...]
    first, second = logits[:, 0:1], logits[:, 1:2]
    top = jnp.maximum(first, second)
    first, second = jnp.exp(first - top), jnp.exp(second - top)
    weighted = picks[0] * (first / (first + second)) + picks[1] * (second / (first + second))
    for s in range(2):
        at_slot = (earlier == float(s)).astype(F32)
        place_scr[s] = transposed(either * at_slot)
        mix_scr[s] = weighted * at_slot

    for s in range(2):
        hz_out[:, s, :] = jnp.dot(
            place_scr[s].astype(BF16), own_scr[...].astype(BF16), preferred_element_type=F32
        )

    tri_scr[:, 0:128] = (iota((128, 128), 0) > iota((128, 128), 1)).astype(BF16)
    tri_scr[:, 128:256] = jnp.ones((128, 128), BF16)

    row_of = iota((padded, 128), 0)
    length_of = jnp.zeros((padded, 128), jnp.int32)
    for b in range(sequences):
        length_of = jnp.where(row_of == b, lengths_ref[b], length_of)

    pl.semaphore_wait(barrier, ep_count + tp_count - 2)

    def far_first(step):
        odd = lax.rem(step, 2)
        off = half + (1 - odd) * (step // 2) - odd * ((step + 1) // 2)
        return lax.rem(place + off, chips)

    def wq_copy(owner, target, sem, slot):
        return pltpu.make_async_remote_copy(
            src_ref=wq_all.at[owner, 0],
            dst_ref=wq_all.at[owner, 0],
            send_sem=send_sem.at[slot],
            recv_sem=sem,
            device_id=(target, mine),
            device_id_type=MESH,
        )

    def wo_copy(owner, target, sem, slot):
        return pltpu.make_async_remote_copy(
            src_ref=wo_all.at[owner],
            dst_ref=wo_all.at[owner],
            send_sem=send_sem.at[slot],
            recv_sem=sem,
            device_id=(target, mine),
            device_id_type=MESH,
        )

    def send_along(copy, recv, slot):
        def step(s, carry):
            copy(me, 2 * far_first(s) + core, recv.at[place], slot).start()
            return carry

        lax.fori_loop(0, chips - 1, step, 0)

    def z_exchange(source, target_ref, sem_at):
        def step(s, carry):
            to = 2 * far_first(s // 2) + lax.rem(s, 2)
            pltpu.make_async_remote_copy(
                src_ref=source.at[to],
                dst_ref=target_ref.at[me],
                send_sem=send_sem.at[sem_at],
                recv_sem=recv_sem.at[sem_at],
                device_id=(to, mine),
                device_id_type=MESH,
            ).start()
            return carry

        lax.fori_loop(0, 2 * (chips - 1), step, 0)
        pltpu.make_async_remote_copy(
            src_ref=source.at[partner],
            dst_ref=target_ref.at[me],
            send_sem=send_sem.at[sem_at],
            recv_sem=recv_sem.at[sem_at],
            device_id=(partner, mine),
            device_id_type=MESH,
        ).start()

    def tp_exchange(source, target_ref, sem_at, scatter):
        def step(d, carry):
            to = lax.rem(mine + d, tp_count)
            pltpu.make_async_remote_copy(
                src_ref=source.at[to] if scatter else source.at[mine],
                dst_ref=target_ref.at[mine],
                send_sem=send_sem.at[sem_at],
                recv_sem=recv_sem.at[sem_at],
                device_id=(me, to),
                device_id_type=MESH,
            ).start()
            return carry

        lax.fori_loop(1, tp_count, step, 0)

    def bytes_of(ref, count, sem):
        some = ref.at[pl.ds(0, count)]
        pltpu.make_async_copy(some, some, sem).wait()

    WQ_RELAY, WO_RELAY, HZ, HR, RS, ASQ, AZ, AR, EX, BACK, CSQ = range(11)
    WQ_SEND, WO_SEND = 11, 12

    send_along(wq_copy, wq_recv, WQ_SEND)
    wq_copy(me, partner, recv_sem.at[WQ_RELAY], WQ_RELAY).start()
    send_along(wo_copy, wo_recv, WO_SEND)
    wo_copy(me, partner, recv_sem.at[WO_RELAY], WO_RELAY).start()
    z_exchange(hz_out, hz_in, HZ)

    def relay(copy, recv, slot):
        def step(d, carry):
            off = (d + 1) // 2
            odd = lax.rem(d, 2)
            source = lax.rem(place + odd * off + (1 - odd) * (chips - off), chips)
            owner = 2 * source + core
            copy(owner, partner, recv.at[source], slot).wait_recv()
            copy(owner, partner, recv_sem.at[slot], slot).start()
            return carry

        lax.fori_loop(1, chips, step, 0)

    relay(wq_copy, wq_recv, WQ_RELAY)
    bytes_of(wq_all.at[:, 0], chips, recv_sem.at[WQ_RELAY])

    for i in range(ep_count):
        wq_all[i, 1] = pltpu.roll(wq_all[i, 0].astype(F32), 64, 1).astype(BF16)
    queries = jnp.dot(
        normed, wq_all[...].reshape(features, 128), preferred_element_type=F32
    )[:, 0:head_size]
    query_columns = transposed(queries)

    loads[0].wait()
    for b in range(sequences):
        product = keys[b].astype(F32) * query_columns[:, b : b + 1]
        scores_scr[b : b + 1, :] = jnp.sum(product, axis=0, keepdims=True)
    bias = stick_bias_ref[0]
    fails, log_hits, insides = [], [], []
    for c in range(blocks):
        score = scores_scr[:, 128 * c : 128 * c + 128] * head_size ** (-0.5) + bias
        inside = iota((padded, 128), 1) + 128 * c < length_of
        soft = jnp.log1p(jnp.exp(-jnp.abs(score)))
        log_hits.append(jnp.minimum(score, 0.0) - soft)
        fails.append(jnp.where(inside, jnp.minimum(-score, 0.0) - soft, 0.0))
        insides.append(inside)
    stacked = jnp.concatenate(fails, axis=0)
    sums = jnp.dot(
        jnp.concatenate(three_parts(stacked), axis=0), tri_scr[...], preferred_element_type=F32
    )
    count = padded * blocks
    sums = (sums[2 * count :] + sums[count : 2 * count]) + sums[:count]
    later = jnp.zeros((padded, 128), F32)
    for c in reversed(range(blocks)):
        block = sums[padded * c : padded * c + padded]
        after = block[:, 0:128] + later
        stick_scr[:, 128 * c : 128 * c + 128] = jnp.where(
            insides[c], jnp.exp(log_hits[c] + after), 0.0
        ).astype(BF16)
        later = later + block[:, 128:256]

    loads[1].wait()
    read = lax.dot_general(
        values[...].reshape(sequences * head_size, positions),
        stick_scr[...],
        NT,
        preferred_element_type=F32,
    )
    column = iota((head_size, padded), 1)
    mixed_columns = jnp.zeros((head_size, padded), F32)
    for b in range(sequences):
        mixed_columns = jnp.where(
            column == b, read[head_size * b : head_size * b + head_size], mixed_columns
        )
    mixed = transposed(mixed_columns).astype(BF16)

    relay(wo_copy, wo_recv, WO_RELAY)
    bytes_of(wo_all, chips, recv_sem.at[WO_RELAY])
    left = iota((wo_half, 128), 1) < 64
    for c in range(chips):
        one, two = wo_all[2 * c].astype(F32), wo_all[2 * c + 1].astype(F32)
        columns = slice(128 * c, 128 * c + 128)
        wo_full[0:wo_half, columns] = jnp.where(left, one, pltpu.roll(two, 64, 1)).astype(BF16)
        wo_full[wo_half : 2 * wo_half, columns] = jnp.where(
            left, pltpu.roll(one, 64, 1), two
        ).astype(BF16)
    for c in range(tp_count):
        rs_out[c] = jnp.dot(
            mixed, wo_full[:, width * c : width * c + width], preferred_element_type=F32
        ).astype(BF16)
    tp_exchange(rs_out, rs_in, RS, True)
    rs_in[mine] = rs_out[mine]

    bytes_of(hz_in, ep_count - 1, recv_sem.at[HZ])
    hz_in[me] = hz_out[me]
    h_rows[mine] = jnp.concatenate([hz_in[:, 0, :], hz_in[:, 1, :]], axis=0).astype(BF16)
    tp_exchange(h_rows, h_rows, HR, False)

    bytes_of(rs_in, tp_count - 1, recv_sem.at[RS])
    total = rs_in[0].astype(F32)
    for c in range(1, tp_count):
        total = total + rs_in[c].astype(F32)
    attended = total.astype(BF16)

    for s in range(2):
        az_out[:, s, :] = jnp.dot(
            place_scr[s].astype(BF16), attended, preferred_element_type=F32
        )
    z_exchange(az_out, az_in, AZ)
    az_in[me] = az_out[me]

    diagonal = iota((padded, 128), 0) == iota((padded, 128), 1)

    def as_row(value):
        return jnp.sum(
            jnp.where(diagonal, jnp.sum(value * value, axis=1, keepdims=True), 0.0),
            axis=0,
            keepdims=True,
        )

    def as_column(row):
        return jnp.sum(jnp.where(diagonal, row, 0.0), axis=1, keepdims=True)

    attended = attended.astype(F32)
    asq_in[mine] = as_row(attended)
    tp_exchange(asq_in, asq_in, ASQ, False)
    bytes_of(h_rows, tp_count - 1, recv_sem.at[HR])

    bytes_of(az_in, ep_count - 1, recv_sem.at[AZ])
    a_rows[mine] = jnp.concatenate([az_in[:, 0, :], az_in[:, 1, :]], axis=0).astype(BF16)
    tp_exchange(a_rows, a_rows, AR, False)

    bytes_of(asq_in, tp_count - 1, recv_sem.at[ASQ])
    squares = as_column(jnp.sum(asq_in[:, 0, :], axis=0, keepdims=True))
    own_gain = gain_scr[mine]
    own_scr[...] = (
        (own_scr[...] + attended * inverse_rms(squares, features) * own_gain)
        .astype(BF16)
        .astype(F32)
    )
    for load in loads[2:]:
        load.wait()

    bytes_of(a_rows, tp_count - 1, recv_sem.at[AR])
    rows = 2 * ep_count
    post_gain = post_gain_ref[...].astype(F32).reshape(1, features)
    ffn_gain = ffn_gain_ref[...].astype(F32).reshape(1, features)
    square = jnp.zeros((rows, width), F32)
    for c in range(tp_count):
        one = a_rows[c].astype(F32)
        square = square + one * one
    scale = inverse_rms(jnp.sum(square, axis=1, keepdims=True), features)
    square = jnp.zeros((rows, width), F32)
    for c in range(tp_count):
        columns = slice(width * c, width * c + width)
        one = (
            h_rows[c].astype(F32) + a_rows[c].astype(F32) * scale * post_gain[:, columns]
        ).astype(BF16)
        r_scr[c] = one
        one = one.astype(F32)
        square = square + one * one
    scale = inverse_rms(jnp.sum(square, axis=1, keepdims=True), features)
    for c in range(tp_count):
        columns = slice(width * c, width * c + width)
        f_scr[:, columns] = (r_scr[c].astype(F32) * scale * ffn_gain[:, columns]).astype(BF16)
    ffn_in = f_scr[...]
    gate_act = jnp.dot(ffn_in, gates[...], preferred_element_type=F32)
    up_act = jnp.dot(ffn_in, ups[...], preferred_element_type=F32)
    active = (gate_act / (1.0 + jnp.exp(-gate_act)) * up_act).astype(BF16)
    for c in range(tp_count):
        ex_out[c] = jnp.dot(
            active, downs[:, width * c : width * c + width], preferred_element_type=F32
        ).astype(BF16)
    tp_exchange(ex_out, ex_in, EX, True)
    ex_in[mine] = ex_out[mine]
    bytes_of(ex_in, tp_count - 1, recv_sem.at[EX])
    total = ex_in[0].astype(F32)
    for c in range(1, tp_count):
        total = total + ex_in[c].astype(F32)
    total = total.astype(BF16).astype(F32)

    for s in range(2):
        back_out[:, s, :] = total[ep_count * s : ep_count * s + ep_count]
    z_exchange(back_out, back_in, BACK)
    back_in[me] = back_out[me]
    bytes_of(back_in, ep_count - 1, recv_sem.at[BACK])
    combined = jnp.zeros((padded, width), F32)
    for s in range(2):
        table = back_in[:, s, :].astype(BF16)
        for part in reversed(three_parts(mix_scr[s])):
            combined = combined + jnp.dot(part, table, preferred_element_type=F32)

    csq_in[mine] = as_row(combined)
    tp_exchange(csq_in, csq_in, CSQ, False)

    bytes_of(wq_all.at[:, 0], chips - 1, send_sem.at[WQ_SEND])
    bytes_of(wq_all.at[:, 0], chips, send_sem.at[WQ_RELAY])
    bytes_of(wo_all, chips - 1, send_sem.at[WO_SEND])
    bytes_of(wo_all, chips, send_sem.at[WO_RELAY])
    for ref, slot in ((hz_out, HZ), (az_out, AZ), (back_out, BACK)):
        bytes_of(ref, ep_count - 1, send_sem.at[slot])
    for ref, slot in (
        (rs_out, RS),
        (h_rows, HR),
        (asq_in, ASQ),
        (a_rows, AR),
        (ex_out, EX),
    ):
        bytes_of(ref, tp_count - 1, send_sem.at[slot])

    bytes_of(csq_in, tp_count - 1, recv_sem.at[CSQ])
    squares = as_column(jnp.sum(csq_in[:, 0, :], axis=0, keepdims=True))
    out_gain = out_gain_ref[...].astype(F32).reshape(1, width)
    result = own_scr[...] + combined * inverse_rms(squares, features) * out_gain
    result_ref[...] = result[0:sequences].astype(BF16)
    bytes_of(csq_in, tp_count - 1, send_sem.at[CSQ])


def per_device(
    hidden,
    pre_gain,
    query_weight,
    key_cache,
    value_cache,
    lengths,
    stick_bias,
    out_weight,
    post_gain,
    ffn_gain,
    expert_ids,
    route_logits,
    gate_experts,
    up_experts,
    down_experts,
    out_gain,
):
    ep_count = lax.axis_size("ep")
    tp_count = lax.axis_size("tp")
    sequences, features = hidden.shape
    positions = key_cache.shape[2]
    width = features // tp_count
    chips = ep_count // 2
    rows = 2 * ep_count
    vmem = pl.BlockSpec(memory_space=pltpu.VMEM)
    smem = pl.BlockSpec(memory_space=pltpu.SMEM)
    hbm = pl.BlockSpec(memory_space=pl.ANY)
    scratch = [
        pltpu.VMEM(key_cache.shape, BF16),
        pltpu.VMEM(value_cache.shape, BF16),
        pltpu.VMEM(gate_experts.shape[1:], BF16),
        pltpu.VMEM(up_experts.shape[1:], BF16),
        pltpu.VMEM(down_experts.shape[1:], BF16),
        pltpu.VMEM((ep_count, 2, 32, 128), BF16),
        pltpu.VMEM((ep_count, 32, 128), BF16),
        pltpu.VMEM((64, features), BF16),
        pltpu.VMEM((16, positions), F32),
        pltpu.VMEM((16, positions), BF16),
        pltpu.VMEM((2, ep_count, 16), F32),
        pltpu.VMEM((2, 16, ep_count), F32),
        pltpu.VMEM((16, 2), jnp.int32),
        pltpu.VMEM((16, 2), F32),
        pltpu.VMEM((16, width), F32),
        pltpu.VMEM((tp_count, 1, width), F32),
        pltpu.VMEM((128, 256), BF16),
        pltpu.VMEM((tp_count, 16, width), BF16),
        pltpu.VMEM((tp_count, 16, width), BF16),
        pltpu.VMEM((ep_count, 2, width), F32),
        pltpu.VMEM((ep_count, 2, width), F32),
        pltpu.VMEM((ep_count, 2, width), F32),
        pltpu.VMEM((ep_count, 2, width), F32),
        pltpu.VMEM((tp_count, rows, width), BF16),
        pltpu.VMEM((tp_count, rows, width), BF16),
        pltpu.VMEM((tp_count, rows, width), BF16),
        pltpu.VMEM((rows, features), BF16),
        pltpu.VMEM((tp_count, rows, width), BF16),
        pltpu.VMEM((tp_count, rows, width), BF16),
        pltpu.VMEM((ep_count, 2, width), F32),
        pltpu.VMEM((ep_count, 2, width), F32),
        pltpu.VMEM((tp_count, 1, width), F32),
        pltpu.VMEM((tp_count, 1, width), F32),
        pltpu.SemaphoreType.DMA((5,)),
        pltpu.SemaphoreType.DMA((chips,)),
        pltpu.SemaphoreType.DMA((chips,)),
        pltpu.SemaphoreType.DMA((13,)),
        pltpu.SemaphoreType.DMA((13,)),
    ]
    return pl.pallas_call(
        functools.partial(layer_kernel, ep_count, tp_count),
        out_shape=jax.ShapeDtypeStruct((sequences, width), BF16),
        in_specs=[
            vmem,
            vmem,
            vmem,
            hbm,
            hbm,
            smem,
            smem,
            vmem,
            vmem,
            vmem,
            vmem,
            vmem,
            hbm,
            hbm,
            hbm,
            vmem,
        ],
        out_specs=vmem,
        scratch_shapes=scratch,
        compiler_params=pltpu.CompilerParams(collective_id=0, has_side_effects=True),
        name="layer",
    )(
        hidden,
        pre_gain,
        query_weight,
        key_cache,
        value_cache,
        lengths,
        stick_bias,
        out_weight,
        post_gain,
        ffn_gain,
        expert_ids,
        route_logits,
        gate_experts,
        up_experts,
        down_experts,
        out_gain,
    )


def solution(mesh):
    placed = (
        P("ep", None),
        P(),
        P("ep", "tp"),
        P("ep", "tp", None),
        P("ep", "tp", None),
        P("ep"),
        P("tp"),
        P("tp", "ep"),
        P(),
        P(),
        P("ep", None),
        P("ep", None),
        P("ep", None, "tp"),
        P("ep", None, "tp"),
        P("ep", "tp", None),
        P("tp"),
    )
    return jax.shard_map(
        per_device, mesh=mesh, in_specs=placed, out_specs=P("ep", "tp"), check_vma=False
    )
```

```python
import functools

import jax
import jax.numpy as jnp
from jax import lax
from jax.experimental import pallas as pl
from jax.experimental.pallas import tpu as pltpu
from jax.sharding import PartitionSpec as P

epsilon = 1e-06
F32 = jnp.float32
BF16 = jnp.bfloat16
MESH = pl.DeviceIdType.MESH
NT = (((1,), (1,)), ((), ()))


def iota(shape, dim):
    return lax.broadcasted_iota(jnp.int32, shape, dim)


def inverse_rms(squares, features):
    return lax.rsqrt(squares / features + epsilon)


def eye(n):
    return (iota((n, n), 0) == iota((n, n), 1)).astype(BF16)


def transposed(value):
    return lax.dot_general(
        eye(value.shape[1]), value.astype(BF16), NT, preferred_element_type=F32
    )


def three_parts(value):
    high = value.astype(BF16)
    rest = value - high.astype(F32)
    middle = rest.astype(BF16)
    low = (rest - middle.astype(F32)).astype(BF16)
    return high, middle, low


def layer_kernel(
    ep_count,
    tp_count,
    hidden_hbm,
    pre_gain_hbm,
    query_weight_hbm,
    key_hbm,
    value_hbm,
    lengths_hbm,
    stick_bias_hbm,
    out_weight_hbm,
    post_gain_hbm,
    ffn_gain_hbm,
    expert_ids_hbm,
    route_logits_hbm,
    gate_hbm,
    up_hbm,
    down_hbm,
    out_gain_hbm,
    result_ref,
    hidden_ref,
    pre_gain_ref,
    query_weight_ref,
    lengths_ref,
    stick_bias_ref,
    out_weight_ref,
    post_gain_ref,
    ffn_gain_ref,
    expert_ids_ref,
    route_logits_ref,
    out_gain_ref,
    keys,
    values,
    gates,
    ups,
    downs,
    wq_all,
    wo_all,
    wo_full,
    scores_scr,
    stick_scr,
    place_scr,
    mix_scr,
    own_scr,
    gain_scr,
    tri_scr,
    rs_out,
    rs_in,
    hz_out,
    hz_in,
    az_out,
    az_in,
    h_rows,
    a_rows,
    r_scr,
    f_scr,
    ex_out,
    ex_in,
    back_out,
    back_in,
    asq_in,
    csq_in,
    load_sem,
    small_sem,
    wq_recv,
    wo_recv,
    recv_sem,
    send_sem,
):
    me = lax.axis_index("ep")
    mine = lax.axis_index("tp")
    place = me // 2
    core = lax.rem(me, 2)
    partner = me + 1 - 2 * core
    chips = ep_count // 2
    half = chips // 2
    reach = chips // 4
    sequences, features = hidden_ref.shape
    padded = 16
    positions = keys.shape[2]
    head_size = keys.shape[1]
    width = features // tp_count
    blocks = positions // 128

    barrier = pltpu.get_barrier_semaphore()

    def greet(target):
        pl.semaphore_signal(barrier, inc=1, device_id=target, device_id_type=MESH)

    def chip_at(off):
        return lax.rem(place + off % chips, chips)

    def greet_tp(d, carry):
        greet((me, lax.rem(mine + d, tp_count)))
        return carry

    for off in range(1, reach + 1):
        greet((2 * chip_at(off) + core, mine))
        greet((2 * chip_at(-off) + core, mine))
    greet((partner, mine))
    lax.fori_loop(1, tp_count, greet_tp, 0)

    smalls = [
        pltpu.make_async_copy(source, target, small_sem.at[at])
        for at, (source, target) in enumerate(
            (
                (query_weight_hbm, query_weight_ref),
                (out_weight_hbm, out_weight_ref),
                (hidden_hbm, hidden_ref),
                (pre_gain_hbm, pre_gain_ref),
                (expert_ids_hbm, expert_ids_ref),
                (route_logits_hbm, route_logits_ref),
                (lengths_hbm, lengths_ref),
                (stick_bias_hbm, stick_bias_ref),
                (post_gain_hbm, post_gain_ref),
                (ffn_gain_hbm, ffn_gain_ref),
                (out_gain_hbm, out_gain_ref),
            )
        )
    ]
    loads = [
        pltpu.make_async_copy(key_hbm, keys, load_sem.at[0]),
        pltpu.make_async_copy(value_hbm, values, load_sem.at[1]),
        pltpu.make_async_copy(gate_hbm.at[0], gates, load_sem.at[2]),
        pltpu.make_async_copy(up_hbm.at[0], ups, load_sem.at[3]),
        pltpu.make_async_copy(down_hbm.at[0], downs, load_sem.at[4]),
    ]
    for load in smalls + loads:
        load.start()
    for load in smalls:
        load.wait()

    wq = query_weight_ref[...].astype(F32)
    rows_half = wq.shape[0] // 2
    wq_all[me, 0] = jnp.concatenate([wq[:rows_half], wq[rows_half:]], axis=1).astype(BF16)
    wo = out_weight_ref[...].astype(F32)
    wo_half = wo.shape[0] // 2
    wo_all[me] = jnp.concatenate([wo[:wo_half], wo[wo_half:]], axis=1).astype(BF16)

    hidden = hidden_ref[...].astype(F32)
    normed = (
        hidden
        * inverse_rms(jnp.sum(hidden * hidden, axis=1, keepdims=True), features)
        * pre_gain_ref[...].astype(F32).reshape(1, features)
    ).astype(BF16)

    own_columns = pl.ds(pl.multiple_of(mine * width, width), width)
    own_scr[...] = hidden_ref[:, own_columns].astype(F32)
    scores_scr[...] = jnp.zeros_like(scores_scr)
    post_gain = post_gain_ref[...].astype(F32).reshape(1, features)
    for c in range(tp_count):
        gain_scr[c] = post_gain[:, width * c : width * c + width]

    ids = expert_ids_ref[...]
    names = iota((ep_count, sequences), 0)
    picks = [(ids[k : k + 1, :] == names).astype(F32) for k in range(2)]
    either = picks[0] + picks[1]
    before = (iota((sequences, sequences), 0) < iota((sequences, sequences), 1)).astype(BF16)
    earlier = jnp.dot(either.astype(BF16), before, preferred_element_type=F32)
    logits = route_logits_ref[...]
    first, second = logits[0:1, :], logits[1:2, :]
    top = jnp.maximum(first, second)
    first, second = jnp.exp(first - top), jnp.exp(second - top)
    weighted = picks[0] * (first / (first + second)) + picks[1] * (second / (first + second))
    for s in range(2):
        at_slot = (earlier == float(s)).astype(F32)
        place_scr[s] = (either * at_slot).astype(BF16)
        for part, value in enumerate(three_parts(weighted * at_slot)):
            mix_scr[s, part] = transposed(value).astype(BF16)

    for s in range(2):
        hz_out[:, s, :] = jnp.dot(
            place_scr[s], own_scr[...].astype(BF16), preferred_element_type=F32
        )

    tri_scr[:, 0:128] = (iota((128, 128), 0) > iota((128, 128), 1)).astype(BF16)
    tri_scr[:, 128:256] = jnp.ones((128, 128), BF16)

    row_of = iota((padded, 128), 0)
    length_of = jnp.zeros((padded, 128), jnp.int32)
    for b in range(sequences):
        length_of = jnp.where(row_of == b, lengths_ref[b], length_of)

    pl.semaphore_wait(barrier, 2 * reach + tp_count)

    def far_first(step):
        odd = lax.rem(step, 2)
        off = half + (1 - odd) * (step // 2) - odd * ((step + 1) // 2)
        return lax.rem(place + off, chips)

    def wq_copy(owner, target, sem, slot):
        return pltpu.make_async_remote_copy(
            src_ref=wq_all.at[owner, 0],
            dst_ref=wq_all.at[owner, 0],
            send_sem=send_sem.at[slot],
            recv_sem=sem,
            device_id=(target, mine),
            device_id_type=MESH,
        )

    def wo_copy(owner, target, sem, slot):
        return pltpu.make_async_remote_copy(
            src_ref=wo_all.at[owner],
            dst_ref=wo_all.at[owner],
            send_sem=send_sem.at[slot],
            recv_sem=sem,
            device_id=(target, mine),
            device_id_type=MESH,
        )

    def send_near(copy, recv, slot):
        for off in range(reach, 0, -1):
            copy(me, 2 * chip_at(off) + core, recv.at[place], slot).start()
            copy(me, 2 * chip_at(-off) + core, recv.at[place], slot).start()

    def send_on(copy, recv, slot):
        for sign, count in ((1, reach), (-1, reach - 1)):
            source = chip_at(-sign * reach)
            owner = 2 * source + core
            copy(owner, partner, recv.at[source], slot).wait_recv()
            for off in range(count, 0, -1):
                copy(owner, 2 * chip_at(sign * off) + core, recv.at[source], slot).start()

    def hand_over(copy, recv, slot, offs, waited):
        for off in offs:
            source = chip_at(off)
            owner = 2 * source + core
            if off not in waited:
                copy(owner, partner, recv.at[source], slot).wait_recv()
            copy(owner, partner, recv_sem.at[slot], slot).start()

    edge = (-reach, reach)
    near = edge + tuple(sign * off for off in range(reach - 1, 0, -1) for sign in (-1, 1))
    far = tuple(sign * off for off in range(reach + 1, half) for sign in (-1, 1)) + (half,)

    def z_exchange(source, target_ref, sem_at):
        def step(s, carry):
            to = 2 * far_first(s // 2) + lax.rem(s, 2)
            pltpu.make_async_remote_copy(
                src_ref=source.at[to],
                dst_ref=target_ref.at[me],
                send_sem=send_sem.at[sem_at],
                recv_sem=recv_sem.at[sem_at],
                device_id=(to, mine),
                device_id_type=MESH,
            ).start()
            return carry

        lax.fori_loop(0, 2 * (chips - 1), step, 0)
        pltpu.make_async_remote_copy(
            src_ref=source.at[partner],
            dst_ref=target_ref.at[me],
            send_sem=send_sem.at[sem_at],
            recv_sem=recv_sem.at[sem_at],
            device_id=(partner, mine),
            device_id_type=MESH,
        ).start()

    def tp_exchange(source, target_ref, sem_at, scatter):
        def step(d, carry):
            to = lax.rem(mine + d, tp_count)
            pltpu.make_async_remote_copy(
                src_ref=source.at[to] if scatter else source.at[mine],
                dst_ref=target_ref.at[mine],
                send_sem=send_sem.at[sem_at],
                recv_sem=recv_sem.at[sem_at],
                device_id=(me, to),
                device_id_type=MESH,
            ).start()
            return carry

        lax.fori_loop(1, tp_count, step, 0)

    def bytes_of(ref, count, sem):
        some = ref.at[pl.ds(0, count)]
        pltpu.make_async_copy(some, some, sem).wait()

    WQ_RELAY, WO_RELAY, HZ, HR, RS, ASQ, AZ, AR, EX, BACK, CSQ = range(11)
    WQ_SEND, WO_SEND = 11, 12

    send_near(wq_copy, wq_recv, WQ_SEND)
    send_near(wo_copy, wo_recv, WO_SEND)
    wq_copy(me, partner, recv_sem.at[WQ_RELAY], WQ_RELAY).start()
    wo_copy(me, partner, recv_sem.at[WO_RELAY], WO_RELAY).start()
    send_on(wq_copy, wq_recv, WQ_SEND)
    send_on(wo_copy, wo_recv, WO_SEND)
    hand_over(wq_copy, wq_recv, WQ_RELAY, near, edge)
    hand_over(wo_copy, wo_recv, WO_RELAY, near, edge)
    hand_over(wq_copy, wq_recv, WQ_RELAY, far, ())
    bytes_of(wq_all.at[:, 0], chips, recv_sem.at[WQ_RELAY])

    for i in range(ep_count):
        wq_all[i, 1] = pltpu.roll(wq_all[i, 0].astype(F32), 64, 1).astype(BF16)
    queries = jnp.dot(
        normed, wq_all[...].reshape(features, 128), preferred_element_type=F32
    )[:, 0:head_size]
    query_columns = transposed(queries)

    loads[0].wait()
    for b in range(sequences):
        product = keys[b].astype(F32) * query_columns[:, b : b + 1]
        scores_scr[b : b + 1, :] = jnp.sum(product, axis=0, keepdims=True)
    bias = stick_bias_ref[0]
    fails, log_hits, insides = [], [], []
    for c in range(blocks):
        score = scores_scr[:, 128 * c : 128 * c + 128] * head_size ** (-0.5) + bias
        inside = iota((padded, 128), 1) + 128 * c < length_of
        soft = jnp.log1p(jnp.exp(-jnp.abs(score)))
        log_hits.append(jnp.minimum(score, 0.0) - soft)
        fails.append(jnp.where(inside, jnp.minimum(-score, 0.0) - soft, 0.0))
        insides.append(inside)
    stacked = jnp.concatenate(fails, axis=0)
    sums = jnp.dot(
        jnp.concatenate(three_parts(stacked), axis=0), tri_scr[...], preferred_element_type=F32
    )
    count = padded * blocks
    sums = (sums[2 * count :] + sums[count : 2 * count]) + sums[:count]
    later = jnp.zeros((padded, 128), F32)
    for c in reversed(range(blocks)):
        block = sums[padded * c : padded * c + padded]
        after = block[:, 0:128] + later
        stick_scr[:, 128 * c : 128 * c + 128] = jnp.where(
            insides[c], jnp.exp(log_hits[c] + after), 0.0
        ).astype(BF16)
        later = later + block[:, 128:256]

    loads[1].wait()
    read = lax.dot_general(
        values[...].reshape(sequences * head_size, positions),
        stick_scr[...],
        NT,
        preferred_element_type=F32,
    )
    column = iota((head_size, padded), 1)
    mixed_columns = jnp.zeros((head_size, padded), F32)
    for b in range(sequences):
        mixed_columns = jnp.where(
            column == b, read[head_size * b : head_size * b + head_size], mixed_columns
        )
    mixed = transposed(mixed_columns).astype(BF16)

    hand_over(wo_copy, wo_recv, WO_RELAY, far, ())
    bytes_of(wo_all, chips, recv_sem.at[WO_RELAY])
    left = iota((wo_half, 128), 1) < 64
    for c in range(chips):
        one, two = wo_all[2 * c].astype(F32), wo_all[2 * c + 1].astype(F32)
        columns = slice(128 * c, 128 * c + 128)
        wo_full[0:wo_half, columns] = jnp.where(left, one, pltpu.roll(two, 64, 1)).astype(BF16)
        wo_full[wo_half : 2 * wo_half, columns] = jnp.where(
            left, pltpu.roll(one, 64, 1), two
        ).astype(BF16)
    for c in range(tp_count):
        rs_out[c] = jnp.dot(
            mixed, wo_full[:, width * c : width * c + width], preferred_element_type=F32
        ).astype(BF16)
    tp_exchange(rs_out, rs_in, RS, True)
    rs_in[mine] = rs_out[mine]
    z_exchange(hz_out, hz_in, HZ)

    bytes_of(rs_in, tp_count - 1, recv_sem.at[RS])
    total = rs_in[0].astype(F32)
    for c in range(1, tp_count):
        total = total + rs_in[c].astype(F32)
    attended = total[0:sequences].astype(BF16)

    for s in range(2):
        az_out[:, s, :] = jnp.dot(
            place_scr[s], attended, preferred_element_type=F32
        )
    z_exchange(az_out, az_in, AZ)
    az_in[me] = az_out[me]

    diagonal = iota((sequences, 128), 0) == iota((sequences, 128), 1)

    def as_row(value):
        return jnp.sum(
            jnp.where(diagonal, jnp.sum(value * value, axis=1, keepdims=True), 0.0),
            axis=0,
            keepdims=True,
        )

    def as_column(row):
        return jnp.sum(jnp.where(diagonal, row, 0.0), axis=1, keepdims=True)

    attended = attended.astype(F32)
    asq_in[mine] = as_row(attended)
    tp_exchange(asq_in, asq_in, ASQ, False)

    bytes_of(hz_in, ep_count - 1, recv_sem.at[HZ])
    hz_in[me] = hz_out[me]
    h_rows[mine] = jnp.concatenate([hz_in[:, 0, :], hz_in[:, 1, :]], axis=0).astype(BF16)
    tp_exchange(h_rows, h_rows, HR, False)

    bytes_of(az_in, ep_count - 1, recv_sem.at[AZ])
    a_rows[mine] = jnp.concatenate([az_in[:, 0, :], az_in[:, 1, :]], axis=0).astype(BF16)
    tp_exchange(a_rows, a_rows, AR, False)

    bytes_of(asq_in, tp_count - 1, recv_sem.at[ASQ])
    squares = as_column(jnp.sum(asq_in[:, 0, :], axis=0, keepdims=True))
    own_gain = gain_scr[mine]
    own_scr[...] = (
        (own_scr[...] + attended * inverse_rms(squares, features) * own_gain)
        .astype(BF16)
        .astype(F32)
    )
    for load in loads[2:]:
        load.wait()

    bytes_of(h_rows, tp_count - 1, recv_sem.at[HR])
    bytes_of(a_rows, tp_count - 1, recv_sem.at[AR])
    rows = 2 * ep_count
    post_gain = post_gain_ref[...].astype(F32).reshape(1, features)
    ffn_gain = ffn_gain_ref[...].astype(F32).reshape(1, features)
    square = jnp.zeros((rows, width), F32)
    for c in range(tp_count):
        one = a_rows[c].astype(F32)
        square = square + one * one
    scale = inverse_rms(jnp.sum(square, axis=1, keepdims=True), features)
    square = jnp.zeros((rows, width), F32)
    for c in range(tp_count):
        columns = slice(width * c, width * c + width)
        one = (
            h_rows[c].astype(F32) + a_rows[c].astype(F32) * scale * post_gain[:, columns]
        ).astype(BF16)
        r_scr[c] = one
        one = one.astype(F32)
        square = square + one * one
    scale = inverse_rms(jnp.sum(square, axis=1, keepdims=True), features)
    for c in range(tp_count):
        columns = slice(width * c, width * c + width)
        f_scr[:, columns] = (r_scr[c].astype(F32) * scale * ffn_gain[:, columns]).astype(BF16)
    ffn_in = f_scr[...]
    gate_act = jnp.dot(ffn_in, gates[...], preferred_element_type=F32)
    up_act = jnp.dot(ffn_in, ups[...], preferred_element_type=F32)
    active = (gate_act / (1.0 + jnp.exp(-gate_act)) * up_act).astype(BF16)
    for c in range(tp_count):
        ex_out[c] = jnp.dot(
            active, downs[:, width * c : width * c + width], preferred_element_type=F32
        ).astype(BF16)
    tp_exchange(ex_out, ex_in, EX, True)
    ex_in[mine] = ex_out[mine]
    bytes_of(ex_in, tp_count - 1, recv_sem.at[EX])
    total = ex_in[0].astype(F32)
    for c in range(1, tp_count):
        total = total + ex_in[c].astype(F32)
    total = total.astype(BF16).astype(F32)

    for s in range(2):
        back_out[:, s, :] = total[ep_count * s : ep_count * s + ep_count]
    z_exchange(back_out, back_in, BACK)
    back_in[me] = back_out[me]
    bytes_of(back_in, ep_count - 1, recv_sem.at[BACK])
    combined = jnp.zeros((sequences, width), F32)
    for s in range(2):
        table = back_in[:, s, :].astype(BF16)
        for part in (2, 1, 0):
            combined = combined + jnp.dot(mix_scr[s, part], table, preferred_element_type=F32)

    csq_in[mine] = as_row(combined)
    tp_exchange(csq_in, csq_in, CSQ, False)

    bytes_of(wq_all.at[:, 0], chips - 1, send_sem.at[WQ_SEND])
    bytes_of(wq_all.at[:, 0], chips, send_sem.at[WQ_RELAY])
    bytes_of(wo_all, chips - 1, send_sem.at[WO_SEND])
    bytes_of(wo_all, chips, send_sem.at[WO_RELAY])
    for ref, slot in ((hz_out, HZ), (az_out, AZ), (back_out, BACK)):
        bytes_of(ref, ep_count - 1, send_sem.at[slot])
    for ref, slot in (
        (rs_out, RS),
        (h_rows, HR),
        (asq_in, ASQ),
        (a_rows, AR),
        (ex_out, EX),
    ):
        bytes_of(ref, tp_count - 1, send_sem.at[slot])

    bytes_of(csq_in, tp_count - 1, recv_sem.at[CSQ])
    squares = as_column(jnp.sum(csq_in[:, 0, :], axis=0, keepdims=True))
    out_gain = out_gain_ref[...].astype(F32).reshape(1, width)
    result = own_scr[...] + combined * inverse_rms(squares, features) * out_gain
    result_ref[...] = result.astype(BF16)
    bytes_of(csq_in, tp_count - 1, send_sem.at[CSQ])


def per_device(
    hidden,
    pre_gain,
    query_weight,
    key_cache,
    value_cache,
    lengths,
    stick_bias,
    out_weight,
    post_gain,
    ffn_gain,
    expert_ids,
    route_logits,
    gate_experts,
    up_experts,
    down_experts,
    out_gain,
):
    ep_count = lax.axis_size("ep")
    tp_count = lax.axis_size("tp")
    sequences, features = hidden.shape
    expert_ids, route_logits = expert_ids.T, route_logits.T
    positions = key_cache.shape[2]
    width = features // tp_count
    chips = ep_count // 2
    rows = 2 * ep_count
    small_args = (
        hidden,
        pre_gain,
        query_weight,
        lengths,
        stick_bias,
        out_weight,
        post_gain,
        ffn_gain,
        expert_ids,
        route_logits,
        out_gain,
    )
    scratch = [
        *(
            (pltpu.SMEM if arg is lengths or arg is stick_bias else pltpu.VMEM)(
                arg.shape, arg.dtype
            )
            for arg in small_args
        ),
        pltpu.VMEM(key_cache.shape, BF16),
        pltpu.VMEM(value_cache.shape, BF16),
        pltpu.VMEM(gate_experts.shape[1:], BF16),
        pltpu.VMEM(up_experts.shape[1:], BF16),
        pltpu.VMEM(down_experts.shape[1:], BF16),
        pltpu.VMEM((ep_count, 2, 32, 128), BF16),
        pltpu.VMEM((ep_count, 32, 128), BF16),
        pltpu.VMEM((64, features), BF16),
        pltpu.VMEM((16, positions), F32),
        pltpu.VMEM((16, positions), BF16),
        pltpu.VMEM((2, ep_count, sequences), BF16),
        pltpu.VMEM((2, 3, sequences, ep_count), BF16),
        pltpu.VMEM((sequences, width), F32),
        pltpu.VMEM((tp_count, 1, width), F32),
        pltpu.VMEM((128, 256), BF16),
        pltpu.VMEM((tp_count, 16, width), BF16),
        pltpu.VMEM((tp_count, 16, width), BF16),
        pltpu.VMEM((ep_count, 2, width), F32),
        pltpu.VMEM((ep_count, 2, width), F32),
        pltpu.VMEM((ep_count, 2, width), F32),
        pltpu.VMEM((ep_count, 2, width), F32),
        pltpu.VMEM((tp_count, rows, width), BF16),
        pltpu.VMEM((tp_count, rows, width), BF16),
        pltpu.VMEM((tp_count, rows, width), BF16),
        pltpu.VMEM((rows, features), BF16),
        pltpu.VMEM((tp_count, rows, width), BF16),
        pltpu.VMEM((tp_count, rows, width), BF16),
        pltpu.VMEM((ep_count, 2, width), F32),
        pltpu.VMEM((ep_count, 2, width), F32),
        pltpu.VMEM((tp_count, 1, width), F32),
        pltpu.VMEM((tp_count, 1, width), F32),
        pltpu.SemaphoreType.DMA((5,)),
        pltpu.SemaphoreType.DMA((11,)),
        pltpu.SemaphoreType.DMA((chips,)),
        pltpu.SemaphoreType.DMA((chips,)),
        pltpu.SemaphoreType.DMA((13,)),
        pltpu.SemaphoreType.DMA((13,)),
    ]
    return pl.pallas_call(
        functools.partial(layer_kernel, ep_count, tp_count),
        out_shape=jax.ShapeDtypeStruct((sequences, width), BF16),
        in_specs=[pl.BlockSpec(memory_space=pl.ANY)] * 16,
        out_specs=pl.BlockSpec(memory_space=pltpu.VMEM),
        scratch_shapes=scratch,
        compiler_params=pltpu.CompilerParams(collective_id=0, has_side_effects=True),
        name="layer",
    )(
        hidden,
        pre_gain,
        query_weight,
        key_cache,
        value_cache,
        lengths,
        stick_bias,
        out_weight,
        post_gain,
        ffn_gain,
        expert_ids,
        route_logits,
        gate_experts,
        up_experts,
        down_experts,
        out_gain,
    )


def solution(mesh):
    placed = (
        P("ep", None),
        P(),
        P("ep", "tp"),
        P("ep", "tp", None),
        P("ep", "tp", None),
        P("ep"),
        P("tp"),
        P("tp", "ep"),
        P(),
        P(),
        P("ep", None),
        P("ep", None),
        P("ep", None, "tp"),
        P("ep", None, "tp"),
        P("ep", "tp", None),
        P("tp"),
    )
    return jax.shard_map(
        per_device, mesh=mesh, in_specs=placed, out_specs=P("ep", "tp"), check_vma=False
    )
```

```python
import functools

import jax
import jax.numpy as jnp
from jax import lax
from jax.experimental import pallas as pl
from jax.experimental.pallas import tpu as pltpu
from jax.sharding import PartitionSpec as P

epsilon = 1e-06
F32 = jnp.float32
BF16 = jnp.bfloat16
MESH = pl.DeviceIdType.MESH
NT = (((1,), (1,)), ((), ()))


def iota(shape, dim):
    return lax.broadcasted_iota(jnp.int32, shape, dim)


def inverse_rms(squares, features):
    return lax.rsqrt(squares / features + epsilon)


def eye(n):
    return (iota((n, n), 0) == iota((n, n), 1)).astype(BF16)


def transposed(value):
    return lax.dot_general(
        eye(value.shape[1]), value.astype(BF16), NT, preferred_element_type=F32
    )


def three_parts(value):
    high = value.astype(BF16)
    rest = value - high.astype(F32)
    middle = rest.astype(BF16)
    low = (rest - middle.astype(F32)).astype(BF16)
    return high, middle, low


def layer_kernel(
    ep_count,
    tp_count,
    hidden_hbm,
    pre_gain_hbm,
    query_weight_hbm,
    key_hbm,
    value_hbm,
    lengths_hbm,
    stick_bias_hbm,
    out_weight_hbm,
    post_gain_hbm,
    ffn_gain_hbm,
    expert_ids_hbm,
    route_logits_hbm,
    gate_hbm,
    up_hbm,
    down_hbm,
    out_gain_hbm,
    result_ref,
    hidden_ref,
    pre_gain_ref,
    query_weight_ref,
    lengths_ref,
    stick_bias_ref,
    out_weight_ref,
    post_gain_ref,
    ffn_gain_ref,
    expert_ids_ref,
    route_logits_ref,
    out_gain_ref,
    keys,
    values,
    gates,
    ups,
    downs,
    wq_all,
    wo_all,
    wo_full,
    scores_scr,
    stick_scr,
    place_scr,
    mix_scr,
    own_scr,
    gain_scr,
    tri_scr,
    rs_out,
    rs_in,
    hz_out,
    hz_in,
    az_out,
    az_in,
    h_rows,
    a_rows,
    r_scr,
    f_scr,
    ex_out,
    ex_in,
    back_out,
    back_in,
    asq_in,
    csq_in,
    load_sem,
    small_sem,
    wq_recv,
    wo_recv,
    recv_sem,
    send_sem,
):
    me = lax.axis_index("ep")
    mine = lax.axis_index("tp")
    place = me // 2
    core = lax.rem(me, 2)
    partner = me + 1 - 2 * core
    chips = ep_count // 2
    half = chips // 2
    reach = chips // 4
    sequences, features = hidden_ref.shape
    padded = 16
    positions = keys.shape[2]
    head_size = keys.shape[1]
    width = features // tp_count
    blocks = positions // 128

    barrier = pltpu.get_barrier_semaphore()

    def greet(target):
        pl.semaphore_signal(barrier, inc=1, device_id=target, device_id_type=MESH)

    def chip_at(off):
        return lax.rem(place + off % chips, chips)

    side = 4
    line, spot = mine // side, lax.rem(mine, side)
    steps = sorted(
        ((dy, dx) for dy in range(side) for dx in range(side) if dy + dx > 0),
        key=lambda step: -sum(min(d, side - d) for d in step),
    )
    others = [
        lax.rem(line + dy, side) * side + lax.rem(spot + dx, side) for dy, dx in steps
    ]

    for off in range(1, reach + 1):
        greet((2 * chip_at(off) + core, mine))
        greet((2 * chip_at(-off) + core, mine))
    greet((partner, mine))
    for to in others:
        greet((me, to))

    smalls = [
        pltpu.make_async_copy(source, target, small_sem.at[at])
        for at, (source, target) in enumerate(
            (
                (query_weight_hbm, query_weight_ref),
                (out_weight_hbm, out_weight_ref),
                (hidden_hbm, hidden_ref),
                (pre_gain_hbm, pre_gain_ref),
                (expert_ids_hbm, expert_ids_ref),
                (route_logits_hbm, route_logits_ref),
                (lengths_hbm, lengths_ref),
                (stick_bias_hbm, stick_bias_ref),
                (post_gain_hbm, post_gain_ref),
                (ffn_gain_hbm, ffn_gain_ref),
                (out_gain_hbm, out_gain_ref),
            )
        )
    ]
    loads = [
        pltpu.make_async_copy(key_hbm, keys, load_sem.at[0]),
        pltpu.make_async_copy(value_hbm, values, load_sem.at[1]),
        pltpu.make_async_copy(gate_hbm.at[0], gates, load_sem.at[2]),
        pltpu.make_async_copy(up_hbm.at[0], ups, load_sem.at[3]),
        pltpu.make_async_copy(down_hbm.at[0], downs, load_sem.at[4]),
    ]
    for load in smalls + loads:
        load.start()
    for load in smalls[:2]:
        load.wait()

    wq = query_weight_ref[...].astype(F32)
    rows_half = wq.shape[0] // 2
    wq_all[me, 0] = jnp.concatenate([wq[:rows_half], wq[rows_half:]], axis=1).astype(BF16)
    wo = out_weight_ref[...].astype(F32)
    wo_half = wo.shape[0] // 2
    wo_all[me] = jnp.concatenate([wo[:wo_half], wo[wo_half:]], axis=1).astype(BF16)

    pl.semaphore_wait(barrier, 2 * reach + tp_count)

    def wq_copy(owner, target, sem, slot):
        return pltpu.make_async_remote_copy(
            src_ref=wq_all.at[owner, 0],
            dst_ref=wq_all.at[owner, 0],
            send_sem=send_sem.at[slot],
            recv_sem=sem,
            device_id=(target, mine),
            device_id_type=MESH,
        )

    def wo_copy(owner, target, sem, slot):
        return pltpu.make_async_remote_copy(
            src_ref=wo_all.at[owner],
            dst_ref=wo_all.at[owner],
            send_sem=send_sem.at[slot],
            recv_sem=sem,
            device_id=(target, mine),
            device_id_type=MESH,
        )

    def send_near(copy, recv, slot):
        for off in range(reach, 0, -1):
            copy(me, 2 * chip_at(off) + core, recv.at[place], slot).start()
            copy(me, 2 * chip_at(-off) + core, recv.at[place], slot).start()

    def send_on(copy, recv, slot):
        for sign, count in ((1, reach), (-1, reach - 1)):
            source = chip_at(-sign * reach)
            owner = 2 * source + core
            copy(owner, partner, recv.at[source], slot).wait_recv()
            for off in range(count, 0, -1):
                copy(owner, 2 * chip_at(sign * off) + core, recv.at[source], slot).start()

    def hand_over(copy, recv, slot, offs, waited):
        for off in offs:
            source = chip_at(off)
            owner = 2 * source + core
            if off not in waited:
                copy(owner, partner, recv.at[source], slot).wait_recv()
            copy(owner, partner, recv_sem.at[slot], slot).start()

    edge = (-reach, reach)
    near = edge + tuple(sign * off for off in range(reach - 1, 0, -1) for sign in (-1, 1))
    far = tuple(sign * off for off in range(reach + 1, half) for sign in (-1, 1)) + (half,)

    def z_send(source, target, send_at, recv_at, off, other):
        to = 2 * chip_at(off) + other
        pltpu.make_async_remote_copy(
            src_ref=source(to, off, other),
            dst_ref=target(off),
            send_sem=send_sem.at[send_at],
            recv_sem=recv_sem.at[recv_at],
            device_id=(to, mine),
            device_id_type=MESH,
        ).start()

    def z_offs(offs):
        return sorted(offs, key=lambda off: -min(off % chips, -off % chips))

    def z_all(source, target, send_at, recv_of, offs):
        for off in z_offs(offs):
            if off == 0:
                z_send(source, target, send_at, recv_of(off), off, 1 - core)
            else:
                for other in range(2):
                    z_send(source, target, send_at, recv_of(off), off, other)

    def spread(source, target, send_at, recv_at):
        z_all(
            lambda to, off, other: source.at[to],
            lambda off: target.at[2 * ((reach - off) % chips) + core],
            send_at,
            lambda off: recv_at[(reach - off) % chips // half],
            range(chips),
        )
        target[2 * reach + core] = source[me]

    def rows_of(arrived, at):
        part = slice(ep_count // 2 * at, ep_count // 2 * (at + 1))
        return jnp.concatenate([arrived[part, 0, :], arrived[part, 1, :]], axis=0).astype(BF16)

    def tp_exchange(source, target_ref, sem_at, scatter):
        for to in others:
            pltpu.make_async_remote_copy(
                src_ref=source.at[to] if scatter else source.at[mine],
                dst_ref=target_ref.at[mine],
                send_sem=send_sem.at[sem_at],
                recv_sem=recv_sem.at[sem_at],
                device_id=(me, to),
                device_id_type=MESH,
            ).start()

    def bytes_of(ref, count, sem):
        some = ref.at[pl.ds(0, count)]
        pltpu.make_async_copy(some, some, sem).wait()

    WQ_RELAY, WO_RELAY, WQ_SEND, WO_SEND, HZ, HR, RS, ASQ, BACK, CSQ = range(10)
    AZ, AR, EX = (10, 11), (12, 13), (14, 15)

    send_near(wq_copy, wq_recv, WQ_SEND)
    send_near(wo_copy, wo_recv, WO_SEND)
    wq_copy(me, partner, recv_sem.at[WQ_RELAY], WQ_RELAY).start()
    wo_copy(me, partner, recv_sem.at[WO_RELAY], WO_RELAY).start()
    for load in smalls[2:]:
        load.wait()
    hidden = hidden_ref[...].astype(F32)
    normed = (
        hidden
        * inverse_rms(jnp.sum(hidden * hidden, axis=1, keepdims=True), features)
        * pre_gain_ref[...].astype(F32).reshape(1, features)
    ).astype(BF16)

    own_columns = pl.ds(pl.multiple_of(mine * width, width), width)
    own_scr[...] = hidden_ref[:, own_columns].astype(F32)
    scores_scr[...] = jnp.zeros_like(scores_scr)
    post_gain = post_gain_ref[...].astype(F32).reshape(1, features)
    for c in range(tp_count):
        gain_scr[c] = post_gain[:, width * c : width * c + width]

    ids = expert_ids_ref[...]
    names = iota((ep_count, sequences), 0)
    picks = [(ids[k : k + 1, :] == names).astype(F32) for k in range(2)]
    either = picks[0] + picks[1]
    before = (iota((sequences, sequences), 0) < iota((sequences, sequences), 1)).astype(BF16)
    earlier = jnp.dot(either.astype(BF16), before, preferred_element_type=F32)
    logits = route_logits_ref[...]
    first, second = logits[0:1, :], logits[1:2, :]
    top = jnp.maximum(first, second)
    first, second = jnp.exp(first - top), jnp.exp(second - top)
    weighted = picks[0] * (first / (first + second)) + picks[1] * (second / (first + second))
    for s in range(2):
        at_slot = (earlier == float(s)).astype(F32)
        place_scr[s] = (either * at_slot).astype(BF16)
        for part, value in enumerate(three_parts(weighted * at_slot)):
            mix_scr[s, part] = transposed(value).astype(BF16)

    for s in range(2):
        hz_out[:, s, :] = jnp.dot(
            place_scr[s], own_scr[...].astype(BF16), preferred_element_type=F32
        )

    tri_scr[:, 0:128] = (iota((128, 128), 0) > iota((128, 128), 1)).astype(BF16)
    tri_scr[:, 128:256] = jnp.ones((128, 128), BF16)

    row_of = iota((padded, 128), 0)
    length_of = jnp.zeros((padded, 128), jnp.int32)
    for b in range(sequences):
        length_of = jnp.where(row_of == b, lengths_ref[b], length_of)

    send_on(wq_copy, wq_recv, WQ_SEND)
    send_on(wo_copy, wo_recv, WO_SEND)
    hand_over(wq_copy, wq_recv, WQ_RELAY, near, edge)
    hand_over(wo_copy, wo_recv, WO_RELAY, near, edge)
    hand_over(wq_copy, wq_recv, WQ_RELAY, far, ())
    bytes_of(wq_all.at[:, 0], chips, recv_sem.at[WQ_RELAY])

    for i in range(ep_count):
        wq_all[i, 1] = pltpu.roll(wq_all[i, 0].astype(F32), 64, 1).astype(BF16)
    queries = jnp.dot(
        normed, wq_all[...].reshape(features, 128), preferred_element_type=F32
    )[:, 0:head_size]
    query_columns = transposed(queries)

    loads[0].wait()
    for b in range(sequences):
        product = keys[b].astype(F32) * query_columns[:, b : b + 1]
        scores_scr[b : b + 1, :] = jnp.sum(product, axis=0, keepdims=True)
    hand_over(wo_copy, wo_recv, WO_RELAY, far, ())
    bias = stick_bias_ref[0]
    fails, log_hits, insides = [], [], []
    for c in range(blocks):
        score = scores_scr[:, 128 * c : 128 * c + 128] * head_size ** (-0.5) + bias
        inside = iota((padded, 128), 1) + 128 * c < length_of
        soft = jnp.log1p(jnp.exp(-jnp.abs(score)))
        log_hits.append(jnp.minimum(score, 0.0) - soft)
        fails.append(jnp.where(inside, jnp.minimum(-score, 0.0) - soft, 0.0))
        insides.append(inside)
    stacked = jnp.concatenate(fails, axis=0)
    sums = jnp.dot(
        jnp.concatenate(three_parts(stacked), axis=0), tri_scr[...], preferred_element_type=F32
    )
    count = padded * blocks
    sums = (sums[2 * count :] + sums[count : 2 * count]) + sums[:count]
    later = jnp.zeros((padded, 128), F32)
    for c in reversed(range(blocks)):
        block = sums[padded * c : padded * c + padded]
        after = block[:, 0:128] + later
        stick_scr[:, 128 * c : 128 * c + 128] = jnp.where(
            insides[c], jnp.exp(log_hits[c] + after), 0.0
        ).astype(BF16)
        later = later + block[:, 128:256]

    loads[1].wait()
    read = lax.dot_general(
        values[...].reshape(sequences * head_size, positions),
        stick_scr[...],
        NT,
        preferred_element_type=F32,
    )
    column = iota((head_size, padded), 1)
    mixed_columns = jnp.zeros((head_size, padded), F32)
    for b in range(sequences):
        mixed_columns = jnp.where(
            column == b, read[head_size * b : head_size * b + head_size], mixed_columns
        )
    mixed = transposed(mixed_columns).astype(BF16)

    spread(hz_out, hz_in, HZ, (HZ, HZ))
    bytes_of(wo_all, chips, recv_sem.at[WO_RELAY])
    left = iota((wo_half, 128), 1) < 64
    for c in range(chips):
        one, two = wo_all[2 * c].astype(F32), wo_all[2 * c + 1].astype(F32)
        columns = slice(128 * c, 128 * c + 128)
        wo_full[0:wo_half, columns] = jnp.where(left, one, pltpu.roll(two, 64, 1)).astype(BF16)
        wo_full[wo_half : 2 * wo_half, columns] = jnp.where(
            left, pltpu.roll(one, 64, 1), two
        ).astype(BF16)
    for c in range(tp_count):
        rs_out[c] = jnp.dot(
            mixed, wo_full[:, width * c : width * c + width], preferred_element_type=F32
        ).astype(BF16)
    tp_exchange(rs_out, rs_in, RS, True)
    rs_in[mine] = rs_out[mine]

    bytes_of(rs_in, tp_count - 1, recv_sem.at[RS])
    total = rs_in[0].astype(F32)
    for c in range(1, tp_count):
        total = total + rs_in[c].astype(F32)
    attended = total[0:sequences].astype(BF16)

    for s in range(2):
        az_out[:, s, :] = jnp.dot(
            place_scr[s], attended, preferred_element_type=F32
        )
    spread(az_out, az_in, AZ[0], AZ)

    diagonal = iota((sequences, 128), 0) == iota((sequences, 128), 1)

    def as_row(value):
        return jnp.sum(
            jnp.where(diagonal, jnp.sum(value * value, axis=1, keepdims=True), 0.0),
            axis=0,
            keepdims=True,
        )

    def as_column(row):
        return jnp.sum(jnp.where(diagonal, row, 0.0), axis=1, keepdims=True)

    attended = attended.astype(F32)
    asq_in[mine] = as_row(attended)
    tp_exchange(asq_in, asq_in, ASQ, False)

    bytes_of(hz_in, ep_count - 1, recv_sem.at[HZ])
    for at in range(2):
        h_rows[mine, at] = rows_of(hz_in, at)
    tp_exchange(h_rows, h_rows, HR, False)

    for at in range(2):
        bytes_of(az_in, ep_count // 2 - 1 + at, recv_sem.at[AZ[at]])
        a_rows[at, mine] = rows_of(az_in, at)
        tp_exchange(a_rows.at[at], a_rows.at[at], AR[at], False)

    bytes_of(asq_in, tp_count - 1, recv_sem.at[ASQ])
    squares = as_column(jnp.sum(asq_in[:, 0, :], axis=0, keepdims=True))
    own_gain = gain_scr[mine]
    own_scr[...] = (
        (own_scr[...] + attended * inverse_rms(squares, features) * own_gain)
        .astype(BF16)
        .astype(F32)
    )
    for load in loads[2:]:
        load.wait()

    post_gain = post_gain_ref[...].astype(F32).reshape(1, features)
    ffn_gain = ffn_gain_ref[...].astype(F32).reshape(1, features)

    def expert(at):
        square = jnp.zeros((ep_count, width), F32)
        for c in range(tp_count):
            one = a_rows[at, c].astype(F32)
            square = square + one * one
        scale = inverse_rms(jnp.sum(square, axis=1, keepdims=True), features)
        square = jnp.zeros((ep_count, width), F32)
        for c in range(tp_count):
            columns = slice(width * c, width * c + width)
            one = (
                h_rows[c, at].astype(F32)
                + a_rows[at, c].astype(F32) * scale * post_gain[:, columns]
            ).astype(BF16)
            r_scr[at, c] = one
            one = one.astype(F32)
            square = square + one * one
        scale = inverse_rms(jnp.sum(square, axis=1, keepdims=True), features)
        for c in range(tp_count):
            columns = slice(width * c, width * c + width)
            f_scr[at, :, columns] = (
                r_scr[at, c].astype(F32) * scale * ffn_gain[:, columns]
            ).astype(BF16)
        ffn_in = f_scr[at]
        gate_act = jnp.dot(ffn_in, gates[...], preferred_element_type=F32)
        up_act = jnp.dot(ffn_in, ups[...], preferred_element_type=F32)
        active = (gate_act / (1.0 + jnp.exp(-gate_act)) * up_act).astype(BF16)
        for c in range(tp_count):
            ex_out[at, c] = jnp.dot(
                active, downs[:, width * c : width * c + width], preferred_element_type=F32
            ).astype(BF16)
        tp_exchange(ex_out.at[at], ex_in.at[at], EX[at], True)
        ex_in[at, mine] = ex_out[at, mine]

    bytes_of(h_rows, tp_count - 1, recv_sem.at[HR])
    for at in range(2):
        bytes_of(a_rows.at[at], tp_count - 1, recv_sem.at[AR[at]])
        expert(at)

    for at in range(2):
        bytes_of(ex_in.at[at], tp_count - 1, recv_sem.at[EX[at]])
        total = ex_in[at, 0].astype(F32)
        for c in range(1, tp_count):
            total = total + ex_in[at, c].astype(F32)
        total = total.astype(BF16).astype(F32)
        part = slice(ep_count // 2 * at, ep_count // 2 * (at + 1))
        for s in range(2):
            back_out[part, s, :] = total[ep_count // 2 * s : ep_count // 2 * (s + 1)]
        z_all(
            lambda to, off, other: back_out.at[2 * ((off + reach) % chips) + other],
            lambda off: back_in.at[me],
            BACK,
            lambda off: BACK,
            [(rel - reach) % chips for rel in range(half * at, half * (at + 1))],
        )
    back_in[me] = back_out[2 * reach + core]
    bytes_of(back_in, ep_count - 1, recv_sem.at[BACK])
    combined = jnp.zeros((sequences, width), F32)
    for s in range(2):
        table = back_in[:, s, :].astype(BF16)
        for part in (2, 1, 0):
            combined = combined + jnp.dot(mix_scr[s, part], table, preferred_element_type=F32)

    csq_in[mine] = as_row(combined)
    tp_exchange(csq_in, csq_in, CSQ, False)

    bytes_of(wq_all.at[:, 0], chips - 1, send_sem.at[WQ_SEND])
    bytes_of(wq_all.at[:, 0], chips, send_sem.at[WQ_RELAY])
    bytes_of(wo_all, chips - 1, send_sem.at[WO_SEND])
    bytes_of(wo_all, chips, send_sem.at[WO_RELAY])
    for ref, slot in ((hz_out, HZ), (az_out, AZ[0]), (back_out, BACK)):
        bytes_of(ref, ep_count - 1, send_sem.at[slot])
    for ref, slot in (
        (rs_out, RS),
        (h_rows, HR),
        (asq_in, ASQ),
        (a_rows.at[0], AR[0]),
        (a_rows.at[1], AR[1]),
        (ex_out.at[0], EX[0]),
        (ex_out.at[1], EX[1]),
    ):
        bytes_of(ref, tp_count - 1, send_sem.at[slot])

    bytes_of(csq_in, tp_count - 1, recv_sem.at[CSQ])
    squares = as_column(jnp.sum(csq_in[:, 0, :], axis=0, keepdims=True))
    out_gain = out_gain_ref[...].astype(F32).reshape(1, width)
    result = own_scr[...] + combined * inverse_rms(squares, features) * out_gain
    result_ref[...] = result.astype(BF16)
    bytes_of(csq_in, tp_count - 1, send_sem.at[CSQ])


def per_device(
    hidden,
    pre_gain,
    query_weight,
    key_cache,
    value_cache,
    lengths,
    stick_bias,
    out_weight,
    post_gain,
    ffn_gain,
    expert_ids,
    route_logits,
    gate_experts,
    up_experts,
    down_experts,
    out_gain,
):
    ep_count = lax.axis_size("ep")
    tp_count = lax.axis_size("tp")
    sequences, features = hidden.shape
    expert_ids, route_logits = expert_ids.T, route_logits.T
    positions = key_cache.shape[2]
    width = features // tp_count
    chips = ep_count // 2
    small_args = (
        hidden,
        pre_gain,
        query_weight,
        lengths,
        stick_bias,
        out_weight,
        post_gain,
        ffn_gain,
        expert_ids,
        route_logits,
        out_gain,
    )
    scratch = [
        *(
            (pltpu.SMEM if arg is lengths or arg is stick_bias else pltpu.VMEM)(
                arg.shape, arg.dtype
            )
            for arg in small_args
        ),
        pltpu.VMEM(key_cache.shape, BF16),
        pltpu.VMEM(value_cache.shape, BF16),
        pltpu.VMEM(gate_experts.shape[1:], BF16),
        pltpu.VMEM(up_experts.shape[1:], BF16),
        pltpu.VMEM(down_experts.shape[1:], BF16),
        pltpu.VMEM((ep_count, 2, 32, 128), BF16),
        pltpu.VMEM((ep_count, 32, 128), BF16),
        pltpu.VMEM((64, features), BF16),
        pltpu.VMEM((16, positions), F32),
        pltpu.VMEM((16, positions), BF16),
        pltpu.VMEM((2, ep_count, sequences), BF16),
        pltpu.VMEM((2, 3, sequences, ep_count), BF16),
        pltpu.VMEM((sequences, width), F32),
        pltpu.VMEM((tp_count, 1, width), F32),
        pltpu.VMEM((128, 256), BF16),
        pltpu.VMEM((tp_count, 16, width), BF16),
        pltpu.VMEM((tp_count, 16, width), BF16),
        pltpu.VMEM((ep_count, 2, width), F32),
        pltpu.VMEM((ep_count, 2, width), F32),
        pltpu.VMEM((ep_count, 2, width), F32),
        pltpu.VMEM((ep_count, 2, width), F32),
        pltpu.VMEM((tp_count, 2, ep_count, width), BF16),
        pltpu.VMEM((2, tp_count, ep_count, width), BF16),
        pltpu.VMEM((2, tp_count, ep_count, width), BF16),
        pltpu.VMEM((2, ep_count, features), BF16),
        pltpu.VMEM((2, tp_count, ep_count, width), BF16),
        pltpu.VMEM((2, tp_count, ep_count, width), BF16),
        pltpu.VMEM((ep_count, 2, width), F32),
        pltpu.VMEM((ep_count, 2, width), F32),
        pltpu.VMEM((tp_count, 1, width), F32),
        pltpu.VMEM((tp_count, 1, width), F32),
        pltpu.SemaphoreType.DMA((5,)),
        pltpu.SemaphoreType.DMA((11,)),
        pltpu.SemaphoreType.DMA((chips,)),
        pltpu.SemaphoreType.DMA((chips,)),
        pltpu.SemaphoreType.DMA((16,)),
        pltpu.SemaphoreType.DMA((16,)),
    ]
    return pl.pallas_call(
        functools.partial(layer_kernel, ep_count, tp_count),
        out_shape=pltpu.VMEM((sequences, width), BF16),
        in_specs=[pl.BlockSpec(memory_space=pl.ANY)] * 16,
        out_specs=pl.BlockSpec(memory_space=pltpu.VMEM),
        scratch_shapes=scratch,
        compiler_params=pltpu.CompilerParams(collective_id=0, has_side_effects=True),
        name="layer",
    )(
        hidden,
        pre_gain,
        query_weight,
        key_cache,
        value_cache,
        lengths,
        stick_bias,
        out_weight,
        post_gain,
        ffn_gain,
        expert_ids,
        route_logits,
        gate_experts,
        up_experts,
        down_experts,
        out_gain,
    )


def solution(mesh):
    placed = (
        P("ep", None),
        P(),
        P("ep", "tp"),
        P("ep", "tp", None),
        P("ep", "tp", None),
        P("ep"),
        P("tp"),
        P("tp", "ep"),
        P(),
        P(),
        P("ep", None),
        P("ep", None),
        P("ep", None, "tp"),
        P("ep", None, "tp"),
        P("ep", "tp", None),
        P("tp"),
    )
    return jax.shard_map(
        per_device, mesh=mesh, in_specs=placed, out_specs=P("ep", "tp"), check_vma=False
    )
```

```python
import functools

import jax
import jax.numpy as jnp
from jax import lax
from jax.experimental import pallas as pl
from jax.experimental.pallas import tpu as pltpu
from jax.sharding import PartitionSpec as P

epsilon = 1e-06
F32 = jnp.float32
BF16 = jnp.bfloat16
MESH = pl.DeviceIdType.MESH
NT = (((1,), (1,)), ((), ()))


def iota(shape, dim):
    return lax.broadcasted_iota(jnp.int32, shape, dim)


def inverse_rms(squares, features):
    return lax.rsqrt(squares / features + epsilon)


def eye(n):
    return (iota((n, n), 0) == iota((n, n), 1)).astype(BF16)


def transposed(value):
    return lax.dot_general(
        eye(value.shape[1]), value.astype(BF16), NT, preferred_element_type=F32
    )


def three_parts(value):
    high = value.astype(BF16)
    rest = value - high.astype(F32)
    middle = rest.astype(BF16)
    low = (rest - middle.astype(F32)).astype(BF16)
    return high, middle, low


def layer_kernel(
    ep_count,
    tp_count,
    hidden_hbm,
    pre_gain_hbm,
    query_weight_hbm,
    key_hbm,
    value_hbm,
    lengths_hbm,
    stick_bias_hbm,
    out_weight_hbm,
    post_gain_hbm,
    ffn_gain_hbm,
    expert_ids_hbm,
    route_logits_hbm,
    gate_hbm,
    up_hbm,
    down_hbm,
    out_gain_hbm,
    result_ref,
    hidden_ref,
    pre_gain_ref,
    query_weight_ref,
    lengths_ref,
    stick_bias_ref,
    out_weight_ref,
    post_gain_ref,
    ffn_gain_ref,
    expert_ids_ref,
    route_logits_ref,
    out_gain_ref,
    keys,
    values,
    gates,
    ups,
    downs,
    wq_all,
    wo_all,
    wo_full,
    scores_scr,
    stick_scr,
    place_scr,
    mix_scr,
    own_scr,
    gain_scr,
    tri_scr,
    rs_out,
    rs_in,
    hz_out,
    hz_in,
    az_out,
    az_in,
    h_rows,
    a_rows,
    r_scr,
    f_scr,
    ex_out,
    ex_in,
    back_out,
    back_in,
    asq_in,
    csq_in,
    load_sem,
    weight_sem,
    recv_sem,
    send_sem,
):
    me = lax.axis_index("ep")
    mine = lax.axis_index("tp")
    place = me // 2
    core = lax.rem(me, 2)
    partner = me + 1 - 2 * core
    chips = ep_count // 2
    half = chips // 2
    reach = chips // 4
    sequences, features = hidden_ref.shape
    padded = 16
    positions = keys.shape[2]
    head_size = keys.shape[1]
    width = features // tp_count
    blocks = positions // 128

    barrier = pltpu.get_barrier_semaphore()

    def greet(target):
        pl.semaphore_signal(barrier, inc=1, device_id=target, device_id_type=MESH)

    def chip_at(off):
        return lax.rem(place + off % chips, chips)

    side = 4
    WQ_RELAY, WO_RELAY, HZ, HR, RS, ASQ, BACK, CSQ = range(8)
    AZ, AR, EX = (8, 9), (10, 11), (12, 13)
    WEIGHTS, ROWS, OTHERS = range(3)
    line, spot = mine // side, lax.rem(mine, side)
    steps = sorted(
        ((dy, dx) for dy in range(side) for dx in range(side) if dy + dx > 0),
        key=lambda step: -sum(min(d, side - d) for d in step),
    )
    others = [
        lax.rem(line + dy, side) * side + lax.rem(spot + dx, side) for dy, dx in steps
    ]

    for off in range(1, reach + 1):
        greet((2 * chip_at(off) + core, mine))
        greet((2 * chip_at(-off) + core, mine))
    greet((partner, mine))
    for to in others:
        greet((me, to))

    smalls = [
        pltpu.make_async_copy(source, target, load_sem.at[at])
        for at, (source, target) in enumerate(
            (
                (query_weight_hbm, query_weight_ref),
                (out_weight_hbm, out_weight_ref),
                (hidden_hbm, hidden_ref),
                (pre_gain_hbm, pre_gain_ref),
                (expert_ids_hbm, expert_ids_ref),
                (route_logits_hbm, route_logits_ref),
                (lengths_hbm, lengths_ref),
                (stick_bias_hbm, stick_bias_ref),
                (post_gain_hbm, post_gain_ref),
                (ffn_gain_hbm, ffn_gain_ref),
                (out_gain_hbm, out_gain_ref),
            )
        )
    ]
    loads = [
        pltpu.make_async_copy(key_hbm, keys, load_sem.at[0]),
        pltpu.make_async_copy(value_hbm, values, load_sem.at[1]),
        pltpu.make_async_copy(gate_hbm.at[0], gates, load_sem.at[2]),
        pltpu.make_async_copy(up_hbm.at[0], ups, load_sem.at[3]),
        pltpu.make_async_copy(down_hbm.at[0], downs, load_sem.at[4]),
    ]
    for load in smalls:
        load.start()
    for load in smalls[:2]:
        load.wait()

    def folded(value):
        rows = value.shape[0] // 2
        return jnp.concatenate([value[:rows], value[rows:]], axis=1).astype(BF16)

    wq_all[me, 0] = folded(query_weight_ref[...].astype(F32))
    wo_all[me] = folded(out_weight_ref[...].astype(F32))
    wo_half = out_weight_ref.shape[0] // 2

    pl.semaphore_wait(barrier, 2 * reach + tp_count)

    def weight(view, base, relay_at):
        def copy(owner, target, sem):
            return pltpu.make_async_remote_copy(
                src_ref=view(owner),
                dst_ref=view(owner),
                send_sem=send_sem.at[WEIGHTS],
                recv_sem=sem,
                device_id=(target, mine),
                device_id_type=MESH,
            )

        return copy, base, relay_at

    def send_near(kind):
        copy, base, relay_at = kind
        for off in range(reach, 0, -1):
            edge = off == reach
            copy(me, 2 * chip_at(off) + core, weight_sem.at[base + (0 if edge else 2)]).start()
            copy(me, 2 * chip_at(-off) + core, weight_sem.at[base + (1 if edge else 2)]).start()

    def send_on(kind):
        copy, base, relay_at = kind
        for way, at, count in (
            (1 - 2 * core, core, reach),
            (2 * core - 1, 1 - core, reach - 1),
        ):
            owner = 2 * lax.rem(place - way * reach + chips, chips) + core
            copy(owner, partner, weight_sem.at[base + at]).wait_recv()
            for off in range(count, 0, -1):
                to = lax.rem(place + way * off + chips, chips)
                copy(owner, 2 * to + core, weight_sem.at[base + 3]).start()

    def hand_over(kind, offs):
        copy, base, relay_at = kind
        for off in offs:
            copy(2 * chip_at(off) + core, partner, recv_sem.at[relay_at]).start()

    inner = 2 * (reach - 1)
    near = tuple(sign * off for off in range(reach, 0, -1) for sign in (-1, 1))
    far = tuple(sign * off for off in range(reach + 1, half) for sign in (-1, 1)) + (half,)

    def z_send(source, target, recv_at, off, other):
        to = 2 * chip_at(off) + other
        pltpu.make_async_remote_copy(
            src_ref=source(to, off, other),
            dst_ref=target(off),
            send_sem=send_sem.at[OTHERS],
            recv_sem=recv_sem.at[recv_at],
            device_id=(to, mine),
            device_id_type=MESH,
        ).start()

    def z_offs(offs):
        return sorted(offs, key=lambda off: -min(off % chips, -off % chips))

    def z_all(source, target, recv_of, offs):
        for off in z_offs(offs):
            if off == 0:
                z_send(source, target, recv_of(off), off, 1 - core)
            else:
                for other in range(2):
                    z_send(source, target, recv_of(off), off, other)

    def spread(source, target, recv_at):
        z_all(
            lambda to, off, other: source.at[to],
            lambda off: target.at[2 * ((reach - off) % chips) + core],
            lambda off: recv_at[(reach - off) % chips // half],
            range(chips),
        )
        target[2 * reach + core] = source[me]

    def rows_of(arrived, at):
        part = slice(ep_count // 2 * at, ep_count // 2 * (at + 1))
        return jnp.concatenate([arrived[part, 0, :], arrived[part, 1, :]], axis=0).astype(BF16)

    def tp_exchange(source, target_ref, sem_at, scatter, send_at):
        for to in others:
            pltpu.make_async_remote_copy(
                src_ref=source.at[to] if scatter else source.at[mine],
                dst_ref=target_ref.at[mine],
                send_sem=send_sem.at[send_at],
                recv_sem=recv_sem.at[sem_at],
                device_id=(me, to),
                device_id_type=MESH,
            ).start()

    def bytes_of(ref, count, sem):
        some = ref.at[pl.ds(0, count)]
        pltpu.make_async_copy(some, some, sem).wait()

    wq = weight(lambda owner: wq_all.at[owner, 0], 0, WQ_RELAY)
    wo = weight(lambda owner: wo_all.at[owner], 4, WO_RELAY)

    send_near(wq)
    send_near(wo)
    hand_over(wq, (0,))
    hand_over(wo, (0,))
    for load in smalls[2:]:
        load.wait()
    for load in loads:
        load.start()
    hidden = hidden_ref[...].astype(F32)
    normed = (
        hidden
        * inverse_rms(jnp.sum(hidden * hidden, axis=1, keepdims=True), features)
        * pre_gain_ref[...].astype(F32).reshape(1, features)
    ).astype(BF16)

    own_columns = pl.ds(pl.multiple_of(mine * width, width), width)
    own_scr[...] = hidden_ref[:, own_columns].astype(F32)
    scores_scr[...] = jnp.zeros_like(scores_scr)
    post_gain = post_gain_ref[...].astype(F32).reshape(1, features)
    for c in range(tp_count):
        gain_scr[c] = post_gain[:, width * c : width * c + width]

    ids = expert_ids_ref[...]
    names = iota((ep_count, sequences), 0)
    picks = [(ids[k : k + 1, :] == names).astype(F32) for k in range(2)]
    either = picks[0] + picks[1]
    before = (iota((sequences, sequences), 0) < iota((sequences, sequences), 1)).astype(BF16)
    earlier = jnp.dot(either.astype(BF16), before, preferred_element_type=F32)
    logits = route_logits_ref[...]
    first, second = logits[0:1, :], logits[1:2, :]
    top = jnp.maximum(first, second)
    first, second = jnp.exp(first - top), jnp.exp(second - top)
    weighted = picks[0] * (first / (first + second)) + picks[1] * (second / (first + second))
    for s in range(2):
        at_slot = (earlier == float(s)).astype(F32)
        place_scr[s] = (either * at_slot).astype(BF16)
        for part, value in enumerate(three_parts(weighted * at_slot)):
            mix_scr[s, part] = transposed(value).astype(BF16)

    for s in range(2):
        hz_out[:, s, :] = jnp.dot(
            place_scr[s], own_scr[...].astype(BF16), preferred_element_type=F32
        )

    tri_scr[:, 0:128] = (iota((128, 128), 0) > iota((128, 128), 1)).astype(BF16)
    tri_scr[:, 128:256] = jnp.ones((128, 128), BF16)

    row_of = iota((padded, 128), 0)
    length_of = jnp.zeros((padded, 128), jnp.int32)
    for b in range(sequences):
        length_of = jnp.where(row_of == b, lengths_ref[b], length_of)

    send_on(wq)
    send_on(wo)
    bytes_of(wq_all.at[:, 0], inner, weight_sem.at[2])
    hand_over(wq, near)
    bytes_of(wo_all, inner, weight_sem.at[6])
    hand_over(wo, near)
    bytes_of(wq_all.at[:, 0], len(far), weight_sem.at[3])
    hand_over(wq, far)
    bytes_of(wq_all.at[:, 0], chips, recv_sem.at[WQ_RELAY])
    spread(hz_out, hz_in, (HZ, HZ))

    for i in range(ep_count):
        wq_all[i, 1] = pltpu.roll(wq_all[i, 0].astype(F32), 64, 1).astype(BF16)
    queries = jnp.dot(
        normed, wq_all[...].reshape(features, 128), preferred_element_type=F32
    )[:, 0:head_size]
    query_columns = transposed(queries)

    bytes_of(wo_all, len(far), weight_sem.at[7])
    hand_over(wo, far)

    loads[0].wait()
    for b in range(sequences):
        product = keys[b].astype(F32) * query_columns[:, b : b + 1]
        scores_scr[b : b + 1, :] = jnp.sum(product, axis=0, keepdims=True)
    bias = stick_bias_ref[0]
    fails, log_hits, insides = [], [], []
    for c in range(blocks):
        score = scores_scr[:, 128 * c : 128 * c + 128] * head_size ** (-0.5) + bias
        inside = iota((padded, 128), 1) + 128 * c < length_of
        soft = jnp.log1p(jnp.exp(-jnp.abs(score)))
        log_hits.append(jnp.minimum(score, 0.0) - soft)
        fails.append(jnp.where(inside, jnp.minimum(-score, 0.0) - soft, 0.0))
        insides.append(inside)
    stacked = jnp.concatenate(fails, axis=0)
    sums = jnp.dot(
        jnp.concatenate(three_parts(stacked), axis=0), tri_scr[...], preferred_element_type=F32
    )
    count = padded * blocks
    sums = (sums[2 * count :] + sums[count : 2 * count]) + sums[:count]
    later = jnp.zeros((padded, 128), F32)
    for c in reversed(range(blocks)):
        block = sums[padded * c : padded * c + padded]
        after = block[:, 0:128] + later
        stick_scr[:, 128 * c : 128 * c + 128] = jnp.where(
            insides[c], jnp.exp(log_hits[c] + after), 0.0
        ).astype(BF16).astype(F32)
        later = later + block[:, 128:256]

    loads[1].wait()
    column = iota((head_size, padded), 1)
    mixed_columns = jnp.zeros((head_size, padded), F32)
    for b in range(sequences):
        read = jnp.zeros((head_size, 128), F32)
        for c in range(blocks):
            columns = slice(128 * c, 128 * c + 128)
            read = read + values[b, :, columns].astype(F32) * stick_scr[b : b + 1, columns]
        mixed_columns = jnp.where(
            column == b, jnp.sum(read, axis=1, keepdims=True), mixed_columns
        )
    mixed = transposed(mixed_columns).astype(BF16)

    bytes_of(wo_all, chips, recv_sem.at[WO_RELAY])
    left = iota((wo_half, 128), 1) < 64
    for c in range(chips):
        one, two = wo_all[2 * c].astype(F32), wo_all[2 * c + 1].astype(F32)
        columns = slice(128 * c, 128 * c + 128)
        wo_full[0:wo_half, columns] = jnp.where(left, one, pltpu.roll(two, 64, 1)).astype(BF16)
        wo_full[wo_half : 2 * wo_half, columns] = jnp.where(
            left, pltpu.roll(one, 64, 1), two
        ).astype(BF16)
    for c in range(tp_count):
        rs_out[c] = jnp.dot(
            mixed, wo_full[:, width * c : width * c + width], preferred_element_type=F32
        ).astype(BF16)
    tp_exchange(rs_out, rs_in, RS, True, OTHERS)
    rs_in[mine] = rs_out[mine]

    bytes_of(rs_in, tp_count - 1, recv_sem.at[RS])
    total = rs_in[0].astype(F32)
    for c in range(1, tp_count):
        total = total + rs_in[c].astype(F32)
    attended = total[0:sequences].astype(BF16)

    for s in range(2):
        az_out[:, s, :] = jnp.dot(
            place_scr[s], attended, preferred_element_type=F32
        )
    spread(az_out, az_in, AZ)

    diagonal = iota((sequences, 128), 0) == iota((sequences, 128), 1)

    def as_row(value):
        return jnp.sum(
            jnp.where(diagonal, jnp.sum(value * value, axis=1, keepdims=True), 0.0),
            axis=0,
            keepdims=True,
        )

    def as_column(row):
        return jnp.sum(jnp.where(diagonal, row, 0.0), axis=1, keepdims=True)

    attended = attended.astype(F32)
    asq_in[mine] = as_row(attended)
    tp_exchange(asq_in, asq_in, ASQ, False, OTHERS)

    bytes_of(hz_in, ep_count - 1, recv_sem.at[HZ])
    for at in range(2):
        h_rows[mine, at] = rows_of(hz_in, at)
    tp_exchange(h_rows, h_rows, HR, False, ROWS)

    for at in range(2):
        bytes_of(az_in, ep_count // 2 - 1 + at, recv_sem.at[AZ[at]])
        a_rows[at, mine] = rows_of(az_in, at)
        tp_exchange(a_rows.at[at], a_rows.at[at], AR[at], False, ROWS)

    bytes_of(asq_in, tp_count - 1, recv_sem.at[ASQ])
    squares = as_column(jnp.sum(asq_in[:, 0, :], axis=0, keepdims=True))
    own_gain = gain_scr[mine]
    own_scr[...] = (
        (own_scr[...] + attended * inverse_rms(squares, features) * own_gain)
        .astype(BF16)
        .astype(F32)
    )
    for load in loads[2:]:
        load.wait()

    post_gain = post_gain_ref[...].astype(F32).reshape(1, features)
    ffn_gain = ffn_gain_ref[...].astype(F32).reshape(1, features)

    def expert(at):
        square = jnp.zeros((ep_count, width), F32)
        for c in range(tp_count):
            one = a_rows[at, c].astype(F32)
            square = square + one * one
        scale = inverse_rms(jnp.sum(square, axis=1, keepdims=True), features)
        square = jnp.zeros((ep_count, width), F32)
        for c in range(tp_count):
            columns = slice(width * c, width * c + width)
            one = (
                h_rows[c, at].astype(F32)
                + a_rows[at, c].astype(F32) * scale * post_gain[:, columns]
            ).astype(BF16)
            r_scr[at, c] = one
            one = one.astype(F32)
            square = square + one * one
        scale = inverse_rms(jnp.sum(square, axis=1, keepdims=True), features)
        for c in range(tp_count):
            columns = slice(width * c, width * c + width)
            f_scr[at, :, columns] = (
                r_scr[at, c].astype(F32) * scale * ffn_gain[:, columns]
            ).astype(BF16)
        ffn_in = f_scr[at]
        gate_act = jnp.dot(ffn_in, gates[...], preferred_element_type=F32)
        up_act = jnp.dot(ffn_in, ups[...], preferred_element_type=F32)
        active = (gate_act / (1.0 + jnp.exp(-gate_act)) * up_act).astype(BF16)
        for c in range(tp_count):
            ex_out[at, c] = jnp.dot(
                active, downs[:, width * c : width * c + width], preferred_element_type=F32
            ).astype(BF16)
        tp_exchange(ex_out.at[at], ex_in.at[at], EX[at], True, OTHERS)
        ex_in[at, mine] = ex_out[at, mine]

    bytes_of(h_rows, tp_count - 1, recv_sem.at[HR])
    for at in range(2):
        bytes_of(a_rows.at[at], tp_count - 1, recv_sem.at[AR[at]])
        expert(at)

    for at in range(2):
        bytes_of(ex_in.at[at], tp_count - 1, recv_sem.at[EX[at]])
        total = ex_in[at, 0].astype(F32)
        for c in range(1, tp_count):
            total = total + ex_in[at, c].astype(F32)
        total = total.astype(BF16).astype(F32)
        part = slice(ep_count // 2 * at, ep_count // 2 * (at + 1))
        for s in range(2):
            back_out[part, s, :] = total[ep_count // 2 * s : ep_count // 2 * (s + 1)]
        z_all(
            lambda to, off, other: back_out.at[2 * ((off + reach) % chips) + other],
            lambda off: back_in.at[me],
            lambda off: BACK,
            [(rel - reach) % chips for rel in range(half * at, half * (at + 1))],
        )
    back_in[me] = back_out[2 * reach + core]
    bytes_of(back_in, ep_count - 1, recv_sem.at[BACK])
    combined = jnp.zeros((sequences, width), F32)
    for s in range(2):
        table = back_in[:, s, :].astype(BF16)
        for part in (2, 1, 0):
            combined = combined + jnp.dot(mix_scr[s, part], table, preferred_element_type=F32)

    csq_in[mine] = as_row(combined)
    tp_exchange(csq_in, csq_in, CSQ, False, OTHERS)

    def size(ref, count):
        total = count * ref.dtype.itemsize
        for extent in ref.shape[1:]:
            total *= extent
        return total

    def left(at, *parts):
        row = gates.shape[1] * gates.dtype.itemsize
        bytes_of(gates, sum(size(*part) for part in parts) // row, send_sem.at[at])

    left(WEIGHTS, (wo_all, 2 * (2 * chips - 1)))
    left(ROWS, (h_rows, tp_count - 1), (a_rows.at[0], 2 * (tp_count - 1)))

    bytes_of(csq_in, tp_count - 1, recv_sem.at[CSQ])
    squares = as_column(jnp.sum(csq_in[:, 0, :], axis=0, keepdims=True))
    out_gain = out_gain_ref[...].astype(F32).reshape(1, width)
    result = own_scr[...] + combined * inverse_rms(squares, features) * out_gain
    result_ref[...] = result.astype(BF16)
    left(
        OTHERS,
        (rs_out, tp_count - 1),
        (ex_out.at[0], 2 * (tp_count - 1)),
        (asq_in, 2 * (tp_count - 1)),
        (hz_out, 3 * (ep_count - 1)),
    )


def per_device(
    hidden,
    pre_gain,
    query_weight,
    key_cache,
    value_cache,
    lengths,
    stick_bias,
    out_weight,
    post_gain,
    ffn_gain,
    expert_ids,
    route_logits,
    gate_experts,
    up_experts,
    down_experts,
    out_gain,
):
    ep_count = lax.axis_size("ep")
    tp_count = lax.axis_size("tp")
    sequences, features = hidden.shape
    expert_ids, route_logits = expert_ids.T, route_logits.T
    positions = key_cache.shape[2]
    width = features // tp_count
    chips = ep_count // 2
    small_args = (
        hidden,
        pre_gain,
        query_weight,
        lengths,
        stick_bias,
        out_weight,
        post_gain,
        ffn_gain,
        expert_ids,
        route_logits,
        out_gain,
    )
    scratch = [
        *(
            (pltpu.SMEM if arg is lengths or arg is stick_bias else pltpu.VMEM)(
                arg.shape, arg.dtype
            )
            for arg in small_args
        ),
        pltpu.VMEM(key_cache.shape, BF16),
        pltpu.VMEM(value_cache.shape, BF16),
        pltpu.VMEM(gate_experts.shape[1:], BF16),
        pltpu.VMEM(up_experts.shape[1:], BF16),
        pltpu.VMEM(down_experts.shape[1:], BF16),
        pltpu.VMEM((ep_count, 2, 32, 128), BF16),
        pltpu.VMEM((ep_count, 32, 128), BF16),
        pltpu.VMEM((64, features), BF16),
        pltpu.VMEM((16, positions), F32),
        pltpu.VMEM((16, positions), F32),
        pltpu.VMEM((2, ep_count, sequences), BF16),
        pltpu.VMEM((2, 3, sequences, ep_count), BF16),
        pltpu.VMEM((sequences, width), F32),
        pltpu.VMEM((tp_count, 1, width), F32),
        pltpu.VMEM((128, 256), BF16),
        pltpu.VMEM((tp_count, 16, width), BF16),
        pltpu.VMEM((tp_count, 16, width), BF16),
        pltpu.VMEM((ep_count, 2, width), F32),
        pltpu.VMEM((ep_count, 2, width), F32),
        pltpu.VMEM((ep_count, 2, width), F32),
        pltpu.VMEM((ep_count, 2, width), F32),
        pltpu.VMEM((tp_count, 2, ep_count, width), BF16),
        pltpu.VMEM((2, tp_count, ep_count, width), BF16),
        pltpu.VMEM((2, tp_count, ep_count, width), BF16),
        pltpu.VMEM((2, ep_count, features), BF16),
        pltpu.VMEM((2, tp_count, ep_count, width), BF16),
        pltpu.VMEM((2, tp_count, ep_count, width), BF16),
        pltpu.VMEM((ep_count, 2, width), F32),
        pltpu.VMEM((ep_count, 2, width), F32),
        pltpu.VMEM((tp_count, 1, width), F32),
        pltpu.VMEM((tp_count, 1, width), F32),
        pltpu.SemaphoreType.DMA((11,)),
        pltpu.SemaphoreType.DMA((8,)),
        pltpu.SemaphoreType.DMA((14,)),
        pltpu.SemaphoreType.DMA((3,)),
    ]
    return pl.pallas_call(
        functools.partial(layer_kernel, ep_count, tp_count),
        out_shape=pltpu.VMEM((sequences, width), BF16),
        in_specs=[pl.BlockSpec(memory_space=pl.ANY)] * 16,
        out_specs=pl.BlockSpec(memory_space=pltpu.VMEM),
        scratch_shapes=scratch,
        compiler_params=pltpu.CompilerParams(collective_id=0, has_side_effects=True),
        name="layer",
    )(
        hidden,
        pre_gain,
        query_weight,
        key_cache,
        value_cache,
        lengths,
        stick_bias,
        out_weight,
        post_gain,
        ffn_gain,
        expert_ids,
        route_logits,
        gate_experts,
        up_experts,
        down_experts,
        out_gain,
    )


def solution(mesh):
    placed = (
        P("ep", None),
        P(),
        P("ep", "tp"),
        P("ep", "tp", None),
        P("ep", "tp", None),
        P("ep"),
        P("tp"),
        P("tp", "ep"),
        P(),
        P(),
        P("ep", None),
        P("ep", None),
        P("ep", None, "tp"),
        P("ep", None, "tp"),
        P("ep", "tp", None),
        P("tp"),
    )
    return jax.shard_map(
        per_device, mesh=mesh, in_specs=placed, out_specs=P("ep", "tp"), check_vma=False
    )
```

```python
import functools

import jax
import jax.numpy as jnp
from jax import lax
from jax.experimental import pallas as pl
from jax.experimental.pallas import tpu as pltpu
from jax.sharding import PartitionSpec as P

epsilon = 1e-06
F32 = jnp.float32
BF16 = jnp.bfloat16
MESH = pl.DeviceIdType.MESH
NT = (((1,), (1,)), ((), ()))


def iota(shape, dim):
    return lax.broadcasted_iota(jnp.int32, shape, dim)


def inverse_rms(squares, features):
    return lax.rsqrt(squares / features + epsilon)


def eye(n):
    return (iota((n, n), 0) == iota((n, n), 1)).astype(BF16)


def transposed(value):
    return lax.dot_general(
        eye(value.shape[1]), value.astype(BF16), NT, preferred_element_type=F32
    )


def three_parts(value):
    high = value.astype(BF16)
    rest = value - high.astype(F32)
    middle = rest.astype(BF16)
    low = (rest - middle.astype(F32)).astype(BF16)
    return high, middle, low


def layer_kernel(
    ep_count,
    tp_count,
    hidden_hbm,
    pre_gain_hbm,
    query_weight_hbm,
    key_hbm,
    value_hbm,
    lengths_hbm,
    stick_bias_hbm,
    out_weight_hbm,
    post_gain_hbm,
    ffn_gain_hbm,
    expert_ids_hbm,
    route_logits_hbm,
    gate_hbm,
    up_hbm,
    down_hbm,
    out_gain_hbm,
    result_ref,
    hidden_ref,
    pre_gain_ref,
    query_weight_ref,
    lengths_ref,
    stick_bias_ref,
    out_weight_ref,
    post_gain_ref,
    ffn_gain_ref,
    expert_ids_ref,
    route_logits_ref,
    out_gain_ref,
    keys,
    values,
    gates,
    ups,
    downs,
    wq_all,
    wo_all,
    norm_scr,
    side_scr,
    scores_scr,
    stick_scr,
    place_scr,
    mix_scr,
    own_scr,
    gain_scr,
    tri_scr,
    rs_out,
    rs_in,
    hz_out,
    hz_in,
    az_out,
    az_in,
    h_rows,
    a_rows,
    f_scr,
    ex_out,
    ex_in,
    back_out,
    back_in,
    asq_in,
    csq_in,
    load_sem,
    weight_sem,
    recv_sem,
    send_sem,
):
    me = lax.axis_index("ep")
    mine = lax.axis_index("tp")
    place = me // 2
    core = lax.rem(me, 2)
    partner = me + 1 - 2 * core
    chips = ep_count // 2
    half = chips // 2
    reach = chips // 4
    sequences, features = hidden_ref.shape
    padded = 16
    positions = keys.shape[2]
    head_size = keys.shape[1]
    width = features // tp_count
    blocks = positions // 128

    barrier = pltpu.get_barrier_semaphore()

    def greet(target):
        pl.semaphore_signal(barrier, inc=1, device_id=target, device_id_type=MESH)

    def chip_at(off):
        return lax.rem(place + off % chips, chips)

    side = 4
    WQ_RELAY, WO_RELAY, HZ, HR, RS, ASQ, BACK, CSQ = range(8)
    AZ, AR, EX = (8, 9), (10, 11), (12, 13)
    WEIGHTS, ROWS, OTHERS = range(3)
    line, column = mine // side, lax.rem(mine, side)
    steps = sorted(
        ((dy, dx) for dy in range(side) for dx in range(side) if dy + dx > 0),
        key=lambda step: -sum(min(d, side - d) for d in step),
    )
    others = [
        lax.rem(line + dy, side) * side + lax.rem(column + dx, side) for dy, dx in steps
    ]

    for off in range(reach, 0, -1):
        greet((2 * chip_at(off) + core, mine))
        greet((2 * chip_at(-off) + core, mine))
    greet((partner, mine))
    for to in others:
        greet((me, to))

    smalls = [
        pltpu.make_async_copy(source, target, load_sem.at[at])
        for at, (source, target) in enumerate(
            (
                (query_weight_hbm, query_weight_ref),
                (out_weight_hbm, out_weight_ref),
                (hidden_hbm, hidden_ref),
                (pre_gain_hbm, pre_gain_ref),
                (expert_ids_hbm, expert_ids_ref),
                (route_logits_hbm, route_logits_ref),
                (lengths_hbm, lengths_ref),
                (stick_bias_hbm, stick_bias_ref),
                (post_gain_hbm, post_gain_ref),
                (ffn_gain_hbm, ffn_gain_ref),
                (out_gain_hbm, out_gain_ref),
            )
        )
    ]
    loads = [
        pltpu.make_async_copy(key_hbm, keys, load_sem.at[0]),
        pltpu.make_async_copy(value_hbm, values, load_sem.at[1]),
        pltpu.make_async_copy(gate_hbm.at[0], gates, load_sem.at[2]),
        pltpu.make_async_copy(up_hbm.at[0], ups, load_sem.at[3]),
        pltpu.make_async_copy(down_hbm.at[0], downs, load_sem.at[4]),
    ]
    for load in smalls:
        load.start()
    for load in smalls[:2]:
        load.wait()

    def folded(value):
        rows = value.shape[0] // 2
        return jnp.concatenate([value[:rows], value[rows:]], axis=1).astype(BF16)

    wq_all[me] = folded(query_weight_ref[...].astype(F32))
    wo_all[me] = folded(out_weight_ref[...].astype(F32))

    pl.semaphore_wait(barrier, 2 * reach + tp_count)

    def weight(view, base, relay_at):
        def copy(owner, target, sem):
            return pltpu.make_async_remote_copy(
                src_ref=view(owner),
                dst_ref=view(owner),
                send_sem=send_sem.at[WEIGHTS],
                recv_sem=sem,
                device_id=(target, mine),
                device_id_type=MESH,
            )

        return copy, base, relay_at

    def send_near(kind):
        copy, base, relay_at = kind
        for off in range(reach, 0, -1):
            edge = off == reach
            copy(me, 2 * chip_at(off) + core, weight_sem.at[base + (0 if edge else 2)]).start()
            copy(me, 2 * chip_at(-off) + core, weight_sem.at[base + (1 if edge else 2)]).start()

    def send_on(kind):
        copy, base, relay_at = kind
        for way, at, count in (
            (1 - 2 * core, core, reach),
            (2 * core - 1, 1 - core, reach - 1),
        ):
            owner = 2 * lax.rem(place - way * reach + chips, chips) + core
            copy(owner, partner, weight_sem.at[base + at]).wait_recv()
            for off in range(count, 0, -1):
                to = lax.rem(place + way * off + chips, chips)
                copy(owner, 2 * to + core, weight_sem.at[base + 3]).start()

    def hand_over(kind, offs):
        copy, base, relay_at = kind
        for off in offs:
            copy(2 * chip_at(off) + core, partner, recv_sem.at[relay_at]).start()

    inner = 2 * (reach - 1)
    near = tuple(sign * off for off in range(reach, 0, -1) for sign in (-1, 1))
    far = tuple(sign * off for off in range(reach + 1, half) for sign in (-1, 1)) + (half,)

    def z_send(source, target, recv_at, off, other):
        to = 2 * chip_at(off) + other
        pltpu.make_async_remote_copy(
            src_ref=source(to, off, other),
            dst_ref=target(off),
            send_sem=send_sem.at[OTHERS],
            recv_sem=recv_sem.at[recv_at],
            device_id=(to, mine),
            device_id_type=MESH,
        ).start()

    def z_offs(offs):
        return sorted(offs, key=lambda off: -min(off % chips, -off % chips))

    def z_all(source, target, recv_of, offs):
        for off in z_offs(offs):
            if off == 0:
                z_send(source, target, recv_of(off), off, 1 - core)
            else:
                for other in range(2):
                    z_send(source, target, recv_of(off), off, other)

    def spread(source, target, recv_at):
        z_all(
            lambda to, off, other: source.at[to],
            lambda off: target.at[2 * ((reach - off) % chips) + core],
            lambda off: recv_at[(reach - off) % chips // half],
            range(chips),
        )
        target[2 * reach + core] = source[me]

    def rows_of(arrived, at):
        part = slice(ep_count // 2 * at, ep_count // 2 * (at + 1))
        return jnp.concatenate([arrived[part, 0, :], arrived[part, 1, :]], axis=0).astype(BF16)

    def tp_exchange(source, target_ref, sem_at, scatter, send_at):
        for to in others:
            pltpu.make_async_remote_copy(
                src_ref=source.at[to] if scatter else source.at[mine],
                dst_ref=target_ref.at[mine],
                send_sem=send_sem.at[send_at],
                recv_sem=recv_sem.at[sem_at],
                device_id=(me, to),
                device_id_type=MESH,
            ).start()

    def bytes_of(ref, count, sem):
        some = ref.at[pl.ds(0, count)]
        pltpu.make_async_copy(some, some, sem).wait()

    wq = weight(lambda owner: wq_all.at[owner], 0, WQ_RELAY)
    wo = weight(lambda owner: wo_all.at[owner], 4, WO_RELAY)

    send_near(wq)
    send_near(wo)
    hand_over(wq, (0,))
    hand_over(wo, (0,))
    for load in smalls[2:]:
        load.wait()
    for load in loads:
        load.start()
    hidden = hidden_ref[...].astype(F32)
    normed = (
        hidden
        * inverse_rms(jnp.sum(hidden * hidden, axis=1, keepdims=True), features)
        * pre_gain_ref[...].astype(F32).reshape(1, features)
    ).astype(BF16)

    norm_scr[...] = jnp.zeros_like(norm_scr)
    for c in range(chips):
        norm_scr[c, 0:sequences, :] = normed[:, 128 * c : 128 * c + 128]
    source, target = iota((128, 128), 0), iota((128, 128), 1)
    piece, upper, spot = source // 64, lax.rem(source // 32, 2), lax.rem(source, 32)
    turned = jnp.dot(
        norm_scr[...].reshape(chips * 16, 128),
        (target == upper * 64 + piece * 32 + spot).astype(BF16),
        preferred_element_type=F32,
    )
    lower = iota((16, 128), 1) < 64
    for c in range(0, chips, 2):
        one, two = turned[16 * c : 16 * c + 16], turned[16 * c + 16 : 16 * c + 32]
        columns = slice(64 * c, 64 * c + 128)
        side_scr[0:16, columns] = jnp.where(lower, one, pltpu.roll(two, 64, 1)).astype(BF16)
        side_scr[16:32, columns] = jnp.where(lower, pltpu.roll(one, 64, 1), two).astype(BF16)

    own_columns = pl.ds(pl.multiple_of(mine * width, width), width)
    own_scr[...] = hidden_ref[:, own_columns].astype(F32)
    scores_scr[...] = jnp.zeros_like(scores_scr)
    post_gain = post_gain_ref[...].astype(F32).reshape(1, features)
    for c in range(tp_count):
        gain_scr[c] = post_gain[:, width * c : width * c + width]

    ids = expert_ids_ref[...]
    names = iota((ep_count, sequences), 0)
    picks = [(ids[k : k + 1, :] == names).astype(F32) for k in range(2)]
    either = picks[0] + picks[1]
    before = (iota((sequences, sequences), 0) < iota((sequences, sequences), 1)).astype(BF16)
    earlier = jnp.dot(either.astype(BF16), before, preferred_element_type=F32)
    logits = route_logits_ref[...]
    first, second = logits[0:1, :], logits[1:2, :]
    top = jnp.maximum(first, second)
    first, second = jnp.exp(first - top), jnp.exp(second - top)
    weighted = picks[0] * (first / (first + second)) + picks[1] * (second / (first + second))
    slots = [(earlier == float(s)).astype(F32) for s in range(2)]
    place_scr[...] = jnp.concatenate([either * slot for slot in slots], axis=0).astype(BF16)
    parts = [part.astype(F32) for slot in slots for part in three_parts(weighted * slot)]
    mix_scr[...] = transposed(jnp.concatenate(parts, axis=0)).astype(BF16)

    def place_rows(target, value):
        placed = jnp.dot(place_scr[...], value, preferred_element_type=F32)
        for s in range(2):
            target[:, s, :] = placed[ep_count * s : ep_count * s + ep_count]

    place_rows(hz_out, own_scr[...].astype(BF16))

    tri_scr[:, 0:128] = (iota((128, 128), 0) > iota((128, 128), 1)).astype(BF16)
    tri_scr[:, 128:256] = jnp.ones((128, 128), BF16)

    row_of = iota((padded, 128), 0)
    length_of = jnp.zeros((padded, 128), jnp.int32)
    for b in range(sequences):
        length_of = jnp.where(row_of == b, lengths_ref[b], length_of)

    send_on(wq)
    send_on(wo)
    bytes_of(wq_all, inner, weight_sem.at[2])
    hand_over(wq, near)
    bytes_of(wo_all, inner, weight_sem.at[6])
    hand_over(wo, near)
    bytes_of(wq_all, len(far), weight_sem.at[3])
    hand_over(wq, far)
    bytes_of(wq_all, chips, recv_sem.at[WQ_RELAY])
    spread(hz_out, hz_in, (HZ, HZ))

    product = jnp.dot(
        side_scr[...], wq_all[...].reshape(features // 2, 128), preferred_element_type=F32
    )
    queries = (product[0:16] + pltpu.roll(product[16:32], 64, 1))[:, 0:head_size]
    query_columns = transposed(queries)

    bytes_of(wo_all, len(far), weight_sem.at[7])
    hand_over(wo, far)

    loads[0].wait()
    for b in range(sequences):
        product = keys[b].astype(F32) * query_columns[:, b : b + 1]
        scores_scr[b : b + 1, :] = jnp.sum(product, axis=0, keepdims=True)
    bias = stick_bias_ref[0]
    fails, log_hits, insides = [], [], []
    for c in range(blocks):
        score = scores_scr[:, 128 * c : 128 * c + 128] * head_size ** (-0.5) + bias
        inside = iota((padded, 128), 1) + 128 * c < length_of
        soft = jnp.log1p(jnp.exp(-jnp.abs(score)))
        log_hits.append(jnp.minimum(score, 0.0) - soft)
        fails.append(jnp.where(inside, jnp.minimum(-score, 0.0) - soft, 0.0))
        insides.append(inside)
    stacked = jnp.concatenate(fails, axis=0)
    sums = jnp.dot(
        jnp.concatenate(three_parts(stacked), axis=0), tri_scr[...], preferred_element_type=F32
    )
    count = padded * blocks
    sums = (sums[2 * count :] + sums[count : 2 * count]) + sums[:count]
    later = jnp.zeros((padded, 128), F32)
    for c in reversed(range(blocks)):
        block = sums[padded * c : padded * c + padded]
        after = block[:, 0:128] + later
        stick_scr[:, 128 * c : 128 * c + 128] = jnp.where(
            insides[c], jnp.exp(log_hits[c] + after), 0.0
        ).astype(BF16).astype(F32)
        later = later + block[:, 128:256]

    loads[1].wait()
    column = iota((head_size, padded), 1)
    mixed_columns = jnp.zeros((head_size, padded), F32)
    for b in range(sequences):
        read = jnp.zeros((head_size, 128), F32)
        for c in range(blocks):
            columns = slice(128 * c, 128 * c + 128)
            read = read + values[b, :, columns].astype(F32) * stick_scr[b : b + 1, columns]
        mixed_columns = jnp.where(
            column == b, jnp.sum(read, axis=1, keepdims=True), mixed_columns
        )
    folds = head_size // 2
    mixed = jnp.concatenate(
        [transposed(mixed_columns[:folds]), transposed(mixed_columns[folds:])], axis=0
    ).astype(BF16)

    bytes_of(wo_all, chips, recv_sem.at[WO_RELAY])
    for c in range(chips):
        one = jnp.dot(mixed, wo_all[2 * c], preferred_element_type=F32)
        two = jnp.dot(mixed, wo_all[2 * c + 1], preferred_element_type=F32)
        swapped = pltpu.roll(jnp.where(lower, two[0:16], one[16:32]), 64, 1)
        rs_out[c] = (jnp.where(lower, one[0:16], two[16:32]) + swapped).astype(BF16)
    tp_exchange(rs_out, rs_in, RS, True, OTHERS)
    rs_in[mine] = rs_out[mine]

    bytes_of(rs_in, tp_count - 1, recv_sem.at[RS])
    total = rs_in[0].astype(F32)
    for c in range(1, tp_count):
        total = total + rs_in[c].astype(F32)
    attended = total[0:sequences].astype(BF16)

    place_rows(az_out, attended)
    spread(az_out, az_in, AZ)

    diagonal = iota((sequences, 128), 0) == iota((sequences, 128), 1)

    def as_row(value):
        return jnp.sum(
            jnp.where(diagonal, jnp.sum(value * value, axis=1, keepdims=True), 0.0),
            axis=0,
            keepdims=True,
        )

    def as_column(row):
        return jnp.sum(jnp.where(diagonal, row, 0.0), axis=1, keepdims=True)

    attended = attended.astype(F32)
    asq_in[mine] = as_row(attended)
    tp_exchange(asq_in, asq_in, ASQ, False, OTHERS)

    bytes_of(hz_in, ep_count - 1, recv_sem.at[HZ])
    for at in range(2):
        h_rows[mine, at] = rows_of(hz_in, at)
    tp_exchange(h_rows, h_rows, HR, False, ROWS)

    for at in range(2):
        bytes_of(az_in, ep_count // 2 - 1 + at, recv_sem.at[AZ[at]])
        a_rows[at, mine] = rows_of(az_in, at)
        tp_exchange(a_rows.at[at], a_rows.at[at], AR[at], False, ROWS)

    bytes_of(asq_in, tp_count - 1, recv_sem.at[ASQ])
    squares = as_column(jnp.sum(asq_in[:, 0, :], axis=0, keepdims=True))
    own_gain = gain_scr[mine]
    own_scr[...] = (
        (own_scr[...] + attended * inverse_rms(squares, features) * own_gain)
        .astype(BF16)
        .astype(F32)
    )
    for load in loads[2:]:
        load.wait()

    post_gain = post_gain_ref[...].astype(F32).reshape(1, features)
    ffn_gain = ffn_gain_ref[...].astype(F32).reshape(1, features)

    def expert(at):
        square = jnp.zeros((ep_count, width), F32)
        for c in range(tp_count):
            one = a_rows[at, c].astype(F32)
            square = square + one * one
        scale = inverse_rms(jnp.sum(square, axis=1, keepdims=True), features)
        square = jnp.zeros((ep_count, width), F32)
        for c in range(tp_count):
            columns = slice(width * c, width * c + width)
            one = (
                h_rows[c, at].astype(F32)
                + a_rows[at, c].astype(F32) * scale * post_gain[:, columns]
            ).astype(BF16)
            one = one.astype(F32)
            square = square + one * one
            f_scr[at, :, columns] = (one * ffn_gain[:, columns]).astype(BF16)
        scale = inverse_rms(jnp.sum(square, axis=1, keepdims=True), features)
        ffn_in = f_scr[at]
        gate_act = jnp.dot(ffn_in, gates[...], preferred_element_type=F32) * scale
        up_act = jnp.dot(ffn_in, ups[...], preferred_element_type=F32) * scale
        active = (gate_act / (1.0 + jnp.exp(-gate_act)) * up_act).astype(BF16)
        for c in range(tp_count):
            ex_out[at, c] = jnp.dot(
                active, downs[:, width * c : width * c + width], preferred_element_type=F32
            ).astype(BF16)
        tp_exchange(ex_out.at[at], ex_in.at[at], EX[at], True, OTHERS)
        ex_in[at, mine] = ex_out[at, mine]

    bytes_of(h_rows, tp_count - 1, recv_sem.at[HR])
    for at in range(2):
        bytes_of(a_rows.at[at], tp_count - 1, recv_sem.at[AR[at]])
        expert(at)

    for at in range(2):
        bytes_of(ex_in.at[at], tp_count - 1, recv_sem.at[EX[at]])
        total = ex_in[at, 0].astype(F32)
        for c in range(1, tp_count):
            total = total + ex_in[at, c].astype(F32)
        total = total.astype(BF16).astype(F32)
        part = slice(ep_count // 2 * at, ep_count // 2 * (at + 1))
        for s in range(2):
            back_out[part, s, :] = total[ep_count // 2 * s : ep_count // 2 * (s + 1)]
        z_all(
            lambda to, off, other: back_out.at[2 * ((off + reach) % chips) + other],
            lambda off: back_in.at[me],
            lambda off: BACK,
            [(rel - reach) % chips for rel in range(half * at, half * (at + 1))],
        )
    back_in[me] = back_out[2 * reach + core]
    bytes_of(back_in, ep_count - 1, recv_sem.at[BACK])
    tables = [back_in[:, s, :].astype(BF16) for s in range(2) for part in range(3)]
    combined = jnp.dot(
        mix_scr[...], jnp.concatenate(tables, axis=0), preferred_element_type=F32
    )

    csq_in[mine] = as_row(combined)
    tp_exchange(csq_in, csq_in, CSQ, False, OTHERS)

    def size(ref, count):
        total = count * ref.dtype.itemsize
        for extent in ref.shape[1:]:
            total *= extent
        return total

    def left(at, *parts):
        row = gates.shape[1] * gates.dtype.itemsize
        bytes_of(gates, sum(size(*part) for part in parts) // row, send_sem.at[at])

    left(WEIGHTS, (wo_all, 2 * (2 * chips - 1)))
    left(ROWS, (h_rows, tp_count - 1), (a_rows.at[0], 2 * (tp_count - 1)))

    bytes_of(csq_in, tp_count - 1, recv_sem.at[CSQ])
    squares = as_column(jnp.sum(csq_in[:, 0, :], axis=0, keepdims=True))
    out_gain = out_gain_ref[...].astype(F32).reshape(1, width)
    result = own_scr[...] + combined * inverse_rms(squares, features) * out_gain
    result_ref[...] = result.astype(BF16)
    left(
        OTHERS,
        (rs_out, tp_count - 1),
        (ex_out.at[0], 2 * (tp_count - 1)),
        (asq_in, 2 * (tp_count - 1)),
        (hz_out, 3 * (ep_count - 1)),
    )


def per_device(
    hidden,
    pre_gain,
    query_weight,
    key_cache,
    value_cache,
    lengths,
    stick_bias,
    out_weight,
    post_gain,
    ffn_gain,
    expert_ids,
    route_logits,
    gate_experts,
    up_experts,
    down_experts,
    out_gain,
):
    ep_count = lax.axis_size("ep")
    tp_count = lax.axis_size("tp")
    sequences, features = hidden.shape
    expert_ids, route_logits = expert_ids.T, route_logits.T
    positions = key_cache.shape[2]
    width = features // tp_count
    chips = ep_count // 2
    small_args = (
        hidden,
        pre_gain,
        query_weight,
        lengths,
        stick_bias,
        out_weight,
        post_gain,
        ffn_gain,
        expert_ids,
        route_logits,
        out_gain,
    )
    scratch = [
        *(
            (pltpu.SMEM if arg is lengths or arg is stick_bias else pltpu.VMEM)(
                arg.shape, arg.dtype
            )
            for arg in small_args
        ),
        pltpu.VMEM(key_cache.shape, BF16),
        pltpu.VMEM(value_cache.shape, BF16),
        pltpu.VMEM(gate_experts.shape[1:], BF16),
        pltpu.VMEM(up_experts.shape[1:], BF16),
        pltpu.VMEM(down_experts.shape[1:], BF16),
        pltpu.VMEM((ep_count, 32, 128), BF16),
        pltpu.VMEM((ep_count, 32, 128), BF16),
        pltpu.VMEM((chips, 16, 128), BF16),
        pltpu.VMEM((32, features // 2), BF16),
        pltpu.VMEM((16, positions), F32),
        pltpu.VMEM((16, positions), F32),
        pltpu.VMEM((2 * ep_count, sequences), BF16),
        pltpu.VMEM((sequences, 6 * ep_count), BF16),
        pltpu.VMEM((sequences, width), F32),
        pltpu.VMEM((tp_count, 1, width), F32),
        pltpu.VMEM((128, 256), BF16),
        pltpu.VMEM((tp_count, 16, width), BF16),
        pltpu.VMEM((tp_count, 16, width), BF16),
        pltpu.VMEM((ep_count, 2, width), F32),
        pltpu.VMEM((ep_count, 2, width), F32),
        pltpu.VMEM((ep_count, 2, width), F32),
        pltpu.VMEM((ep_count, 2, width), F32),
        pltpu.VMEM((tp_count, 2, ep_count, width), BF16),
        pltpu.VMEM((2, tp_count, ep_count, width), BF16),
        pltpu.VMEM((2, ep_count, features), BF16),
        pltpu.VMEM((2, tp_count, ep_count, width), BF16),
        pltpu.VMEM((2, tp_count, ep_count, width), BF16),
        pltpu.VMEM((ep_count, 2, width), F32),
        pltpu.VMEM((ep_count, 2, width), F32),
        pltpu.VMEM((tp_count, 1, width), F32),
        pltpu.VMEM((tp_count, 1, width), F32),
        pltpu.SemaphoreType.DMA((11,)),
        pltpu.SemaphoreType.DMA((8,)),
        pltpu.SemaphoreType.DMA((14,)),
        pltpu.SemaphoreType.DMA((3,)),
    ]
    return pl.pallas_call(
        functools.partial(layer_kernel, ep_count, tp_count),
        out_shape=pltpu.VMEM((sequences, width), BF16),
        in_specs=[pl.BlockSpec(memory_space=pl.ANY)] * 16,
        out_specs=pl.BlockSpec(memory_space=pltpu.VMEM),
        scratch_shapes=scratch,
        compiler_params=pltpu.CompilerParams(collective_id=0, has_side_effects=True),
        name="layer",
    )(
        hidden,
        pre_gain,
        query_weight,
        key_cache,
        value_cache,
        lengths,
        stick_bias,
        out_weight,
        post_gain,
        ffn_gain,
        expert_ids,
        route_logits,
        gate_experts,
        up_experts,
        down_experts,
        out_gain,
    )


def solution(mesh):
    placed = (
        P("ep", None),
        P(),
        P("ep", "tp"),
        P("ep", "tp", None),
        P("ep", "tp", None),
        P("ep"),
        P("tp"),
        P("tp", "ep"),
        P(),
        P(),
        P("ep", None),
        P("ep", None),
        P("ep", None, "tp"),
        P("ep", None, "tp"),
        P("ep", "tp", None),
        P("tp"),
    )
    return jax.shard_map(
        per_device, mesh=mesh, in_specs=placed, out_specs=P("ep", "tp"), check_vma=False
    )
```
